512 devices in a mesh: ep: 32 (over z, x), tp: 16 (over y, core).
Axes of the slice: x: 4, y: 8, z: 8, core: 2. Of those that a mesh axis runs over, the one named last changes fastest.
Arguments:
- queries: bfloat16 [4096, 4096], P('ep', 'tp'), may hold values from -112 to 112
- key_rows: bfloat16 [4096, 4096], P('ep', 'tp'), may hold values from -8.1 to 8.1
- values: bfloat16 [4096, 4096], P('ep', 'tp'), may hold values from -6 to 6
- lambdas: float32 [16], P('tp'), may hold values from 0.3 to 0.8
- head_gain: float32 [256], replicated, may hold values from 0.1 to 1.9
- tokens: bfloat16 [2048, 4096], P('ep'), may hold values from -6 to 6
- moe_gain: float32 [4096], replicated, may hold values from 0.1 to 1.9
- routes: int32 [2048, 2], P('ep'), may hold values from 0 to 31, all different within a row; in each aligned block of 64 rows (0 to 63, 64 to 127, ...) at most 8 rows name the same one
- route_scores: float32 [2048, 2], P('ep'), may hold values from -6 to 6
- w_gate: bfloat16 [32, 4096, 2048], P('ep', None, 'tp'), may hold values from -0.09375 to 0.09375
- w_up: bfloat16 [32, 4096, 2048], P('ep', None, 'tp'), may hold values from -0.09375 to 0.09375
- w_down: bfloat16 [32, 2048, 4096], P('ep', 'tp'), may hold values from -0.125 to 0.125
Outputs:
- attended: bfloat16 [4096, 4096], P('ep', 'tp')
- expert_out: bfloat16 [2048, 4096], P('ep', 'tp')
The draws below stay inside these ranges and needn't reach their ends.
Inputs may be any that keep to these rules, and one draw needn't show every extreme that they name: `routes`: each row names 2 different experts. Among the rows of one index of ep at most 8 name the same expert, and some index reaches 8 in every draw.
All inputs are finite; a program needn't handle non-finite values.
Results may differ from the reference program's by a relative error of at most 0.018.
Values may be sent and summed in bfloat16 or wider, within the bound.
A program may use at most 64 MiB of HBM per device.

```python
import math
from functools import partial
import jax
import jax.numpy as jnp
import numpy as np
from jax import lax

D = 4096
HEADS = 16
QKD = 128
VD = 256
FF = 2048
TOP = 2
TOKB_DEV = 64
SEQ = 4096
TOKB = 2048
EXPERTS = 32
CAP = 8
N_EP = 32
N_TP = 16


def base_pairs(key):
    seed_one, seed_two, seed_three, seed_four, seed_five = jax.random.split(jax.random.fold_in(key, 11), 5)
    row_width = HEADS * 2 * QKD
    queries = jnp.clip(jax.random.normal(seed_one, (SEQ, row_width), jnp.float32) * 1.3, -8.0, 8.0)
    key_rows = jnp.clip(jax.random.normal(seed_two, (SEQ, row_width), jnp.float32) * 1.3, -8.0, 8.0)
    return (queries, key_rows, seed_three, seed_four, seed_five)


def draw_queries(key, part):
    drawn = base_pairs(key)
    return drawn[0].astype(jnp.bfloat16)


def draw_key_rows(key, part):
    drawn = base_pairs(key)
    return drawn[1].astype(jnp.bfloat16)


def block_levels(own_key, shape, cuts, smallest, largest):
    gain = 1.0
    for dim, parts in cuts:
        heights = jax.random.uniform(jax.random.fold_in(jax.random.fold_in(own_key, 6), dim), (parts,), jnp.float32, smallest / len(cuts), largest / len(cuts))
        gain = gain * jnp.repeat(jnp.exp(heights), shape[dim] // parts).reshape((-1,) + (1,) * (len(shape) - 1 - dim))
    return gain


def shared_out(rng, own, number, rows, amount, top, reach, lean):
    ranking = jax.random.permutation(rng, amount)
    heavy_load, usual = shares(amount, rows * top, reach, lean, True), shares(amount, rows * top, reach, lean, False)
    places = jnp.arange(amount)

    def named(tallies, offset_by):
        used = int((tallies > 0).sum())
        fixed = max(1, used // 4)
        passed = fixed + (places - fixed + offset_by * (used - fixed)) % max(1, amount - fixed)
        return jnp.zeros((amount,), jnp.int32).at[ranking[jnp.where(places < fixed, places, passed)]].set(jnp.asarray(tallies, jnp.int32))

    tallies = jnp.where(number % 4 == 0, named(heavy_load, number // 4), named(usual, number - number // 4 - 1))
    mixed = jax.random.permutation(jax.random.fold_in(own, 3), amount)
    giver, sink = mixed[0:amount // 2 * 2:2], mixed[1:amount // 2 * 2:2]
    margin = jnp.minimum(tallies[giver] - 1, reach - tallies[sink]) // 2
    margin = jnp.where((giver == ranking[0]) | (sink == ranking[0]) | (tallies[sink] == 0), 0, jnp.maximum(margin, 0))
    passed = jax.random.randint(jax.random.fold_in(own, 4), (amount // 2,), 0, 1 << 20) % (margin + 1)
    tallies = tallies.at[giver].add(-passed).at[sink].add(passed)
    members = jnp.searchsorted(jnp.cumsum(tallies), jnp.arange(rows * top), side="right").astype(jnp.int32)
    grid = members.reshape(top, rows).T
    grid = grid[jax.random.permutation(jax.random.fold_in(own, 1), rows)]
    offset_by = jax.random.randint(jax.random.fold_in(own, 2), (rows, 1), 0, top)
    return jnp.take_along_axis(grid, (jnp.arange(top)[None, :] + offset_by) % top, axis=1)


def shares(number_of, total, reach, slope, full):
    loads = [(1 << 20) // math.isqrt(standing ** slope) + 1 for standing in range(1, number_of + 1)]
    largest = reach if full else min(reach, max(-(-total // number_of), total * loads[0] // sum(loads)))
    least = 1 if total - largest >= number_of - 1 else 0
    given, spare = [largest] + [least] * (number_of - 1), total - largest - least * (number_of - 1)
    while spare > 0:
        candidates = [i for i in range(1, number_of) if given[i] < largest] or [i for i in range(1, number_of) if given[i] < reach]
        whole, budget = sum([loads[i] for i in candidates]), spare
        for i in candidates:
            extra = min(reach - given[i], max(1, budget * loads[i] // whole), spare)
            given[i] = given[i] + extra
            spare = spare - extra
    return np.array(given)


def bell_draw(own_key, dims, spread, limit, pieces=(), held_as=jnp.bfloat16):
    array = spread * jax.random.normal(own_key, dims, jnp.float32)
    if pieces:
        array = array * block_levels(own_key, dims, pieces, -0.22, 0.18)
    return jnp.clip(array, -limit, limit).astype(held_as)


def setup_inputs(seed: int = 0) -> dict:
    arg_keys = jax.random.split(jax.random.key(seed), 13)
    queries = draw_queries(jax.random.fold_in(arg_keys[12], 71), 0)
    key_rows = draw_key_rows(jax.random.fold_in(arg_keys[12], 71), 0)
    values = bell_draw(arg_keys[2], (SEQ, HEADS * VD), 1.0, 6.0, ((0, 32), (1, 16)))
    lambdas = jnp.clip(0.3 + 0.5 * jax.random.uniform(arg_keys[3], (HEADS,), jnp.float32) ** block_levels(arg_keys[3], (HEADS,), ((0, 16),), -0.2, 0.2), 0.3, 0.8)
    head_gain = jnp.clip(1.0 + 0.18 * jax.random.normal(arg_keys[4], (VD,), jnp.float32), 0.1, 1.9)
    tokens = bell_draw(arg_keys[5], (TOKB, D), 1.0, 6.0, ((0, 32),))
    moe_gain = jnp.clip(1.0 + 0.18 * jax.random.normal(arg_keys[6], (D,), jnp.float32), 0.1, 1.9)
    routes_keys = jax.random.split(jax.random.fold_in(arg_keys[7], 1), TOKB // TOKB_DEV)
    routes_turns = jax.random.permutation(jax.random.fold_in(arg_keys[7], 3), TOKB // TOKB_DEV)
    routes = jax.vmap(lambda own, number: shared_out(jax.random.fold_in(arg_keys[7], 2), own, number, TOKB_DEV, EXPERTS, TOP, CAP, 1))(routes_keys, routes_turns).reshape((TOKB, TOP))
    route_scores = bell_draw(arg_keys[8], (TOKB, TOP), 1.0, 6.0, ((0, 32),), jnp.float32)
    w_gate = bell_draw(arg_keys[9], (EXPERTS, D, FF), D ** -0.5, 0.09375, ((0, 32), (2, 16)))
    w_up = bell_draw(arg_keys[10], (EXPERTS, D, FF), D ** -0.5, 0.09375, ((0, 32), (2, 16)))
    w_down = bell_draw(arg_keys[11], (EXPERTS, FF, D), FF ** -0.5, 0.125, ((0, 32), (1, 16)))
    return {"queries": queries, "key_rows": key_rows, "values": values, "lambdas": lambdas, "head_gain": head_gain, "tokens": tokens, "moe_gain": moe_gain, "routes": routes, "route_scores": route_scores, "w_gate": w_gate, "w_up": w_up, "w_down": w_down}


neg_big = -1e+30
head_eps = 1e-05
moe_eps = 1e-06
head_scale = 0.8

def slot_table(routes, experts, capacity):
    flat_routes = routes.reshape(-1)
    onehot = (flat_routes[:, None] == jnp.arange(experts, dtype=jnp.int32)[None, :]).astype(jnp.int32)
    before = jnp.cumsum(onehot, axis=0) - onehot
    position = lax.optimization_barrier(jnp.sum(before * onehot, axis=1))
    return (flat_routes * capacity + position).astype(jnp.int32).reshape(routes.shape)

def reference(queries, key_rows, values, lambdas, head_gain, tokens, moe_gain, routes, route_scores, w_gate, w_up, w_down):
    query_heads = queries.reshape(SEQ, HEADS, 2, QKD).transpose(1, 0, 2, 3)
    key_heads = key_rows.reshape(SEQ, HEADS, 2, QKD).transpose(1, 0, 2, 3)
    value_heads = values.reshape(SEQ, HEADS, VD).transpose(1, 0, 2)
    visible = jnp.tril(jnp.ones((SEQ, SEQ), dtype=bool))

    def one_head(inputs):
        query_h, key_h, value_h, weight_h = inputs
        scores = jnp.einsum('qmd,kmd->mqk', query_h.astype(jnp.float32), key_h.astype(jnp.float32), precision=lax.Precision.HIGHEST) * QKD ** (-0.5)
        scores = jnp.where(visible[None], scores, neg_big)
        probabilities = jax.nn.softmax(scores, axis=-1)
        mixing = probabilities[0] - weight_h * probabilities[1]
        mixed_out = jnp.dot(mixing, value_h.astype(jnp.float32), precision=lax.Precision.HIGHEST)
        scaled = mixed_out * lax.rsqrt(lax.optimization_barrier(jnp.mean(mixed_out * mixed_out, axis=-1, keepdims=True)) + head_eps)
        return (scaled * head_gain * head_scale).astype(jnp.bfloat16)
    heads_out = lax.map(one_head, (query_heads, key_heads, value_heads, lambdas))
    attended = heads_out.transpose(1, 0, 2).reshape(SEQ, HEADS * VD)
    token_f32 = tokens.astype(jnp.float32)
    normed = (token_f32 * lax.rsqrt(lax.optimization_barrier(jnp.mean(token_f32 * token_f32, axis=-1, keepdims=True)) + moe_eps) * moe_gain).astype(jnp.bfloat16)
    gate_weights = jax.nn.softmax(route_scores, axis=-1)
    local_slots = jax.vmap(partial(slot_table, experts=EXPERTS, capacity=CAP))(routes.reshape(N_EP, TOKB_DEV, TOP))
    expert_ids = local_slots // CAP
    within = local_slots % CAP
    source = jnp.arange(N_EP, dtype=jnp.int32)[:, None, None]
    global_slot = (expert_ids * (N_EP * CAP) + source * CAP + within).astype(jnp.int32).reshape(TOKB, TOP)
    row_ids = jnp.broadcast_to(jnp.arange(TOKB, dtype=jnp.int32)[:, None], (TOKB, TOP))
    row_of_slot = jnp.zeros((EXPERTS * N_EP * CAP,), jnp.int32).at[global_slot.reshape(-1)].set(row_ids.reshape(-1))
    gathered = normed[row_of_slot].reshape(EXPERTS, N_EP * CAP, D)
    group_size = FF // N_TP

    def one_expert(inputs):
        rows_e, gate_e, up_e, down_e = inputs
        gate_act = jnp.dot(rows_e, gate_e, preferred_element_type=jnp.float32)
        up_act = jnp.dot(rows_e, up_e, preferred_element_type=jnp.float32)
        hidden = (jax.nn.silu(gate_act) * up_act).astype(jnp.bfloat16)

        def add_group(group_index, running):
            offset = (group_index * group_size).astype(jnp.int32)
            hidden_part = lax.dynamic_slice_in_dim(hidden, offset, group_size, 1)
            down_part = lax.dynamic_slice_in_dim(down_e, offset, group_size, 0)
            partial_sum = jnp.dot(hidden_part, down_part, preferred_element_type=jnp.float32).astype(jnp.bfloat16)
            partial_sum = lax.optimization_barrier(partial_sum)
            return running + partial_sum.astype(jnp.float32)
        running = lax.fori_loop(jnp.int32(0), jnp.int32(N_TP), add_group, jnp.zeros((N_EP * CAP, D), jnp.float32))
        return running.astype(jnp.bfloat16)
    results = lax.map(one_expert, (gathered, w_gate, w_up, w_down)).reshape(EXPERTS * N_EP * CAP, D)
    picked = results[global_slot].astype(jnp.float32)
    expert_out = lax.optimization_barrier(jnp.sum(gate_weights[..., None] * picked, axis=1)).astype(jnp.bfloat16)
    return (attended, expert_out)
```

```python
import jax
import jax.numpy as jnp
from jax import lax
from jax.experimental import pallas as pl
from jax.experimental.pallas import tpu as pltpu
from jax.sharding import PartitionSpec as P

MESH = pl.DeviceIdType.MESH
F32 = jnp.float32
BF16 = jnp.bfloat16

QKD = 128
VD = 256
D = 4096
N_EP = 32
N_TP = 16
NX = 4
RING = 8
CAP = 8
ROWS_A = 128
ROWS_B = 64
SLOTS = N_EP * CAP
FEAT = D // N_TP
FFL = 128
SUB = 4
SROWS = SLOTS // SUB
KSUB = 2
KROWS = ROWS_A // KSUB

neg_big = -1e30
head_eps = 1e-05
moe_eps = 1e-06
head_scale = 0.8


def kernel(
    q_in, k_in, v_in, lam_in, hg_in, tok_in, mg_in, routes_in, rs_in, wg_in, wu_in, wd_in,
    att_out, exp_out,
    tok, small_sem, wsem, outbox, inbox, gath, wgu, wdx, hid, zown, sbuf, rbuf,
    ebox, retbox, qall, kv, osend, ssend, orecv, srecv,
    disp_s, disp_r, ag_s, ag_r, dd_s, dd_r, wdx_s, wdx_r, hid_s, hid_r,
    rsc_s, rsc_r, ret_s, ret_r, q_s, q_r, kv_s, kv_r, o_s, o_r,
):
    ep = lax.axis_index("ep")
    tp = lax.axis_index("tp")
    z, x = lax.div(ep, NX), lax.rem(ep, NX)
    y, core = lax.div(tp, 2), lax.rem(tp, 2)
    mate = (ep, y * 2 + 1 - core)

    def ring(i, d):
        return lax.rem(i + d + RING, RING)

    y_next = ((ep, ring(y, 1) * 2 + core), (ep, ring(y, -1) * 2 + core))
    z_next = ((ring(z, 1) * NX + x, tp), (ring(z, -1) * NX + x, tp))

    def ep_peer(k):
        return lax.rem(ep + k, N_EP)

    def x_peer(k):
        return z * NX + lax.rem(x + k, NX)

    def rdma(src, dst, ssem, rsem, dev):
        return pltpu.make_async_remote_copy(
            src_ref=src, dst_ref=dst, send_sem=ssem, recv_sem=rsem,
            device_id=dev, device_id_type=MESH,
        )

    tok_load = pltpu.make_async_copy(tok_in, tok, small_sem.at[0])
    tok_load.start()
    loads_q = pltpu.make_async_copy(q_in, qall.at[x], small_sem.at[1])
    loads_k = pltpu.make_async_copy(k_in, kv.at[z, :, pl.ds(0, 256)], small_sem.at[2])
    loads_v = pltpu.make_async_copy(v_in, kv.at[z, :, pl.ds(256, 256)], small_sem.at[3])
    loads_q.start()
    loads_k.start()
    loads_v.start()
    load_wg = pltpu.make_async_copy(wg_in.at[0], wgu.at[:, pl.ds(0, FFL)], wsem.at[0])
    load_wu = pltpu.make_async_copy(wu_in.at[0], wgu.at[:, pl.ds(FFL, FFL)], wsem.at[1])
    load_wg.start()
    load_wu.start()

    def wd_cols(yd, c):
        return wd_in.at[0, :, pl.ds(pl.multiple_of((yd * 2 + c) * FEAT, FEAT), FEAT)]

    def wd_load(yd):
        return pltpu.make_async_copy(wd_cols(yd, core), wdx.at[core, yd], wsem.at[2 + yd])

    for yd in range(RING):
        wd_load(yd).start()

    barrier = pltpu.get_barrier_semaphore()

    def greet(k, carry):
        pl.semaphore_signal(barrier, inc=1, device_id=(ep_peer(k), tp), device_id_type=MESH)
        return carry

    lax.fori_loop(1, N_EP, greet, 0)
    for dev in (*y_next, mate):
        pl.semaphore_signal(barrier, inc=1, device_id=dev, device_id_type=MESH)

    r0, r1 = routes_in[:, 0:1], routes_in[:, 1:2]
    lane = lax.broadcasted_iota(jnp.int32, (ROWS_B, 128), 1)
    hit0, hit1 = lane == r0, lane == r1
    named = jnp.where(hit0 | hit1, 1.0, 0.0).astype(BF16)
    row_i = lax.broadcasted_iota(jnp.int32, (ROWS_B, ROWS_B), 0)
    col_i = lax.broadcasted_iota(jnp.int32, (ROWS_B, ROWS_B), 1)
    earlier = jnp.where(col_i < row_i, 1.0, 0.0).astype(BF16)
    before = jnp.dot(earlier, named, preferred_element_type=F32)
    pos0 = jnp.sum(jnp.where(hit0, before, 0.0), axis=1, keepdims=True)
    pos1 = jnp.sum(jnp.where(hit1, before, 0.0), axis=1, keepdims=True)
    slot0 = r0.astype(F32) * CAP + pos0
    slot1 = r1.astype(F32) * CAP + pos1
    slot_lane = lax.broadcasted_iota(jnp.int32, (ROWS_B, SLOTS), 1).astype(F32)
    pick0 = jnp.where(slot_lane == slot0, 1.0, 0.0)
    pick1 = jnp.where(slot_lane == slot1, 1.0, 0.0)
    s0, s1 = rs_in[:, 0:1], rs_in[:, 1:2]
    smax = jnp.maximum(s0, s1)
    g0, g1 = jnp.exp(s0 - smax), jnp.exp(s1 - smax)
    gsum = g0 + g1
    g0, g1 = g0 / gsum, g1 / gsum

    tok_load.wait()
    squares = jnp.zeros((ROWS_B, 256), F32)
    for i in range(D // 256):
        part = tok[:, i * 256:(i + 1) * 256].astype(F32)
        squares = squares + part * part
    mean = jnp.sum(squares, axis=1, keepdims=True) * (1.0 / D)
    cols = pl.ds(pl.multiple_of(tp * FEAT, FEAT), FEAT)
    normed = (tok[:, cols].astype(F32) * lax.rsqrt(mean + moe_eps) * mg_in[:, cols]).astype(BF16)
    outgoing = lax.dot_general(
        (pick0 + pick1).astype(BF16), normed, (((0,), (0,)), ((), ())), preferred_element_type=F32
    )
    outbox[...] = outgoing.reshape(N_EP, CAP, FEAT).astype(BF16)

    pl.semaphore_wait(barrier, N_EP - 1 + 3)

    def dispatch(k, carry):
        peer = ep_peer(k)
        rdma(outbox.at[peer], inbox.at[ep], disp_s, disp_r, (peer, tp)).start()
        return carry

    lax.fori_loop(1, N_EP, dispatch, 0)
    inbox[ep] = outbox[ep]

    wd_pair = [rdma(wd_cols(yd, 1 - core), wdx.at[core, yd], wdx_s.at[yd], wdx_r.at[yd], mate) for yd in range(RING)]
    for copy in wd_pair:
        copy.start()
    loads_q.wait()
    q_copies = [
        rdma(qall.at[x], qall.at[x], q_s.at[k - 1], q_r.at[k - 1], (x_peer(k), tp)) for k in range(1, NX)
    ]
    for copy in q_copies:
        copy.start()
    loads_k.wait()
    loads_v.wait()

    def kv_copy(way, d, j):
        origin = ring(z, -(d - 1) if way == 0 else d - 1)
        piece = kv.at[origin, pl.ds(j * KROWS, KROWS)]
        return rdma(piece, piece, kv_s.at[way, d - 1, j], kv_r.at[way, d - 1, j], z_next[way])

    def travels(way, d, j, pieces):
        return d < 4 or (j < pieces // 2) == (way == 0)

    for j in range(KSUB):
        for way in range(2):
            kv_copy(way, 1, j).start()

    def kv_step(d):
        for j in range(KSUB):
            for way in range(2):
                if travels(way, d, j, KSUB):
                    kv_copy(way, d, j).wait_recv()
                    if d < 4 and travels(way, d + 1, j, KSUB):
                        kv_copy(way, d + 1, j).start()

    whole_in = inbox.at[pl.ds(0, N_EP - 1)]
    rdma(whole_in, whole_in, disp_s, disp_r, mate).wait_recv()
    gath[tp] = inbox[...].astype(F32).reshape(SLOTS, FEAT).astype(BF16)

    def gath_piece(origin, c, j):
        return gath.at[origin * 2 + c, pl.ds(j * SROWS, SROWS)]

    def ag_copy(way, d, j):
        origin = ring(y, -(d - 1) if way == 0 else d - 1)
        piece = gath_piece(origin, core, j)
        return rdma(piece, piece, ag_s.at[way, d - 1, j], ag_r.at[way, d - 1, j], y_next[way])

    def dd_copy(rel, j):
        piece = gath_piece(ring(y, rel), core, j)
        return rdma(piece, piece, dd_s.at[rel, j], dd_r.at[rel, j], mate)

    for j in range(SUB):
        for way in range(2):
            ag_copy(way, 1, j).start()
        dd_copy(0, j).start()
    for d in range(1, 5):
        for j in range(SUB):
            for way in range(2):
                if travels(way, d, j, SUB):
                    ag_copy(way, d, j).wait_recv()
                    if d < 4 and travels(way, d + 1, j, SUB):
                        ag_copy(way, d + 1, j).start()
                    dd_copy((RING - d) if way == 0 else d, j).start()
        kv_step(d)
    for rel in range(RING):
        for j in range(SUB):
            dd_copy(rel, j).wait_recv()
    load_wg.wait()
    load_wu.wait()

    acc = jnp.zeros((SLOTS, 2 * FFL), F32)
    for t in range(N_TP):
        acc = acc + jnp.dot(gath[t], wgu[t * FEAT:(t + 1) * FEAT, :], preferred_element_type=F32)
    gate_act, up_act = acc[:, :FFL], acc[:, FFL:]
    hid[core] = (gate_act * jax.nn.sigmoid(gate_act) * up_act).astype(BF16)
    hid_copy = rdma(hid.at[core], hid.at[core], hid_s, hid_r, mate)
    hid_copy.start()
    for yd in range(RING):
        wd_load(yd).wait()
        wd_pair[yd].wait_recv()
    for copy in q_copies:
        copy.wait_recv()
    hid_copy.wait_recv()

    def attend(xq, m):
        qm = qall[xq, :, m * QKD:(m + 1) * QKD]
        keys = kv[:, :, m * QKD:(m + 1) * QKD].reshape(RING * ROWS_A, QKD)
        vals = kv[:, :, 256:512].reshape(RING * ROWS_A, VD)
        s = lax.dot_general(qm, keys, (((1,), (1,)), ((), ())), preferred_element_type=F32) * QKD ** (-0.5)
        col = lax.broadcasted_iota(jnp.int32, s.shape, 1)
        row = lax.broadcasted_iota(jnp.int32, s.shape, 0)
        key_pos = (col >> 7) * (NX * ROWS_A) + x * ROWS_A + (col & 127)
        visible = key_pos <= row + (z * NX + xq) * ROWS_A
        s = jnp.where(visible, s, neg_big)
        top = jnp.max(s, axis=1, keepdims=True)
        w = jnp.where(visible, jnp.exp(s - top), 0.0)
        total = jnp.sum(w, axis=1, keepdims=True)
        o = jnp.dot(w.astype(BF16), vals, preferred_element_type=F32)
        return o, top, total

    def attend_block(k):
        xq = lax.rem(x + k, NX)
        o0, m0, l0 = attend(xq, 0)
        osend[k, :, 0:VD] = o0.astype(BF16)
        o1, m1, l1 = attend(xq, 1)
        osend[k, :, VD:2 * VD] = o1.astype(BF16)
        sl = lax.broadcasted_iota(jnp.int32, (ROWS_A, 128), 1)
        ssend[k] = jnp.where(sl == 0, m0, jnp.where(sl == 1, l0, jnp.where(sl == 2, m1, l1)))

    def o_copies(k):
        dev = (x_peer(k), tp)
        return (
            rdma(osend.at[k], orecv.at[k - 1], o_s.at[0, k - 1], o_r.at[0, k - 1], dev),
            rdma(ssend.at[k], srecv.at[k - 1], o_s.at[1, k - 1], o_r.at[1, k - 1], dev),
        )

    def attend_step(k):
        attend_block(k)
        if k > 0:
            for copy in o_copies(k):
                copy.start()

    hid0, hid1 = hid[0], hid[1]

    def own_term(rel):
        yd = ring(y, rel)
        zown[rel] = jnp.dot(hid0, wdx[0, yd], preferred_element_type=F32) + jnp.dot(
            hid1, wdx[1, yd], preferred_element_type=F32
        )

    def rel_of(way, r):
        return r % RING if way == 0 else (RING - r) % RING

    def rs_copy(way, r, j):
        rows = pl.ds(j * SROWS, SROWS)
        return rdma(
            sbuf.at[way, r - 1, rows], rbuf.at[way, r - 1, rows],
            rsc_s.at[way, r - 1, j], rsc_r.at[way, r - 1, j], y_next[way],
        )

    def rs_send(way, r, j):
        rows = slice(j * SROWS, (j + 1) * SROWS)
        term = zown[rel_of(way, r), rows, :]
        if r < 4 and travels(way, r + 1, j, SUB):
            rs_copy(way, r + 1, j).wait_recv()
            term = term + rbuf[way, r, rows, :].astype(F32)
        sbuf[way, r - 1, rows, :] = term.astype(BF16)
        rs_copy(way, r, j).start()

    own_term(4)
    for j in range(SUB):
        for way in range(2):
            if travels(way, 4, j, SUB):
                rs_send(way, 4, j)
    own_term(3)
    own_term(5)
    order = {0: list(range(SUB // 2, SUB)) + list(range(SUB // 2)), 1: list(range(SUB))}
    for i in range(SUB):
        for way in range(2):
            rs_send(way, 3, order[way][i])
        if i == SUB // 2 - 1:
            for rel in (2, 6, 1, 7, 0):
                own_term(rel)
            attend_step(1)
    attend_step(2)
    for r in (2, 1):
        for i in range(SUB):
            for way in range(2):
                rs_send(way, r, order[way][i])
        attend_step(3 if r == 2 else 0)
    for j in range(SUB):
        rows = slice(j * SROWS, (j + 1) * SROWS)
        rs_copy(0, 1, j).wait_recv()
        rs_copy(1, 1, j).wait_recv()
        result = zown[0, rows, :] + rbuf[0, 0, rows, :].astype(F32) + rbuf[1, 0, rows, :].astype(F32)
        ebox[j * (SROWS // CAP):(j + 1) * (SROWS // CAP)] = result.reshape(SROWS // CAP, CAP, FEAT).astype(BF16)

    def send_back(k, carry):
        peer = ep_peer(k)
        rdma(ebox.at[peer], retbox.at[ep], ret_s, ret_r, (peer, tp)).start()
        return carry

    lax.fori_loop(1, N_EP, send_back, 0)
    retbox[ep] = ebox[ep]

    for k in range(1, NX):
        for copy in o_copies(k):
            copy.wait_recv()

    def joined(m):
        tops = [ssend[0, :, 2 * m:2 * m + 1]] + [srecv[k, :, 2 * m:2 * m + 1] for k in range(NX - 1)]
        sums = [ssend[0, :, 2 * m + 1:2 * m + 2]] + [srecv[k, :, 2 * m + 1:2 * m + 2] for k in range(NX - 1)]
        outs = [osend[0, :, m * VD:(m + 1) * VD]] + [orecv[k, :, m * VD:(m + 1) * VD] for k in range(NX - 1)]
        top = jnp.maximum(jnp.maximum(tops[0], tops[1]), jnp.maximum(tops[2], tops[3]))
        scale = [jnp.exp(t - top) for t in tops]
        total = sum(f * s for f, s in zip(scale, sums))
        return sum(f * o.astype(F32) for f, o in zip(scale, outs)) / total

    mixed = joined(0) - lam_in[...] * joined(1)
    power = jnp.mean(mixed * mixed, axis=1, keepdims=True)
    att_out[...] = (mixed * lax.rsqrt(power + head_eps) * hg_in[...] * head_scale).astype(BF16)

    whole_ret = retbox.at[pl.ds(0, N_EP - 1)]
    rdma(whole_ret, whole_ret, ret_s, ret_r, mate).wait_recv()
    back = retbox[...].astype(F32).reshape(SLOTS, FEAT).astype(BF16)
    first = jnp.dot(pick0.astype(BF16), back, preferred_element_type=F32)
    second = jnp.dot(pick1.astype(BF16), back, preferred_element_type=F32)
    exp_out[...] = (g0 * first + g1 * second).astype(BF16)

    whole_out = outbox.at[pl.ds(0, N_EP - 1)]
    rdma(whole_out, whole_out, disp_s, disp_r, mate).wait_send()
    whole_e = ebox.at[pl.ds(0, N_EP - 1)]
    rdma(whole_e, whole_e, ret_s, ret_r, mate).wait_send()
    for copy in wd_pair + q_copies + [hid_copy]:
        copy.wait_send()
    for k in range(1, NX):
        for copy in o_copies(k):
            copy.wait_send()
    for way in range(2):
        for d in range(1, 5):
            for j in range(KSUB):
                if travels(way, d, j, KSUB):
                    kv_copy(way, d, j).wait_send()
            for j in range(SUB):
                if travels(way, d, j, SUB):
                    ag_copy(way, d, j).wait_send()
                    rs_copy(way, d, j).wait_send()
    for rel in range(RING):
        for j in range(SUB):
            dd_copy(rel, j).wait_send()


def local(
    queries, key_rows, values, lambdas, head_gain, tokens, moe_gain, routes, route_scores, w_gate, w_up, w_down,
):
    hbm = pl.BlockSpec(memory_space=pl.ANY)
    vmem = pl.BlockSpec(memory_space=pltpu.VMEM)
    dma = pltpu.SemaphoreType.DMA
    scratch = [
        pltpu.VMEM((ROWS_B, D), BF16),
        dma((4,)),
        dma((2 + RING,)),
        pltpu.VMEM((N_EP, CAP, FEAT), BF16),
        pltpu.VMEM((N_EP, CAP, FEAT), BF16),
        pltpu.VMEM((N_TP, SLOTS, FEAT), BF16),
        pltpu.VMEM((D, 2 * FFL), BF16),
        pltpu.VMEM((2, RING, FFL, FEAT), BF16),
        pltpu.VMEM((2, SLOTS, FFL), BF16),
        pltpu.VMEM((RING, SLOTS, FEAT), F32),
        pltpu.VMEM((2, 4, SLOTS, FEAT), BF16),
        pltpu.VMEM((2, 4, SLOTS, FEAT), BF16),
        pltpu.VMEM((N_EP, CAP, FEAT), BF16),
        pltpu.VMEM((N_EP, CAP, FEAT), BF16),
        pltpu.VMEM((NX, ROWS_A, 2 * QKD), BF16),
        pltpu.VMEM((RING, ROWS_A, 512), BF16),
        pltpu.VMEM((NX, ROWS_A, 2 * VD), BF16),
        pltpu.VMEM((NX, ROWS_A, 128), F32),
        pltpu.VMEM((NX - 1, ROWS_A, 2 * VD), BF16),
        pltpu.VMEM((NX - 1, ROWS_A, 128), F32),
        dma, dma,
        dma((2, 4, SUB)), dma((2, 4, SUB)),
        dma((RING, SUB)), dma((RING, SUB)),
        dma((RING,)), dma((RING,)),
        dma, dma,
        dma((2, 4, SUB)), dma((2, 4, SUB)),
        dma, dma,
        dma((NX - 1,)), dma((NX - 1,)),
        dma((2, 4, KSUB)), dma((2, 4, KSUB)),
        dma((2, NX - 1)), dma((2, NX - 1)),
    ]
    return pl.pallas_call(
        kernel,
        out_shape=(
            jax.ShapeDtypeStruct((ROWS_A, VD), BF16),
            jax.ShapeDtypeStruct((ROWS_B, FEAT), BF16),
        ),
        in_specs=[hbm, hbm, hbm, vmem, vmem, hbm, vmem, vmem, vmem, hbm, hbm, hbm],
        out_specs=(vmem, vmem),
        scratch_shapes=scratch,
        compiler_params=pltpu.CompilerParams(
            collective_id=0, has_side_effects=True, vmem_limit_bytes=40 * 1024 * 1024
        ),
    )(
        queries, key_rows, values, lambdas.reshape(1, 1), head_gain.reshape(1, VD), tokens,
        moe_gain.reshape(1, D), routes, route_scores, w_gate, w_up, w_down,
    )


def solution(mesh):
    return jax.shard_map(
        local,
        mesh=mesh,
        in_specs=(
            P("ep", "tp"), P("ep", "tp"), P("ep", "tp"), P("tp"), P(), P("ep", None), P(),
            P("ep", None), P("ep", None), P("ep", None, "tp"), P("ep", None, "tp"), P("ep", "tp", None),
        ),
        out_specs=(P("ep", "tp"), P("ep", "tp")),
        check_vma=False,
    )
```

```python
import jax
import jax.numpy as jnp
from jax import lax
from jax.experimental import pallas as pl
from jax.experimental.pallas import tpu as pltpu
from jax.sharding import PartitionSpec as P

MESH = pl.DeviceIdType.MESH
F32 = jnp.float32
BF16 = jnp.bfloat16

QKD = 128
VD = 256
D = 4096
N_EP = 32
N_TP = 16
NX = 4
RING = 8
CAP = 8
ROWS_A = 128
ROWS_B = 64
SLOTS = N_EP * CAP
FEAT = D // N_TP
FFL = 128
SUB = 4
SROWS = SLOTS // SUB
GSRC = N_EP // SUB
KSUB = 2
KROWS = ROWS_A // KSUB

neg_big = -1e30
head_eps = 1e-05
moe_eps = 1e-06
head_scale = 0.8


def kernel(
    q_in, k_in, v_in, lam_in, hg_in, tok_in, mg_in, routes_in, rs_in, wg_in, wu_in, wd_in,
    att_out, exp_out,
    tok, lam, mg, hg, routes, scores, pick0, pick1, small_sem, wsem,
    outbox, outfar, inbox, infar, gath, acts, wgu, wdx, hid, zown, sbuf, rbuf,
    ebox, retbox, qall, kv, osend, ssend, orecv, srecv,
    disp_s, disp_r, far_s, far_r, ag_s, ag_r, dd_s, dd_r, wdx_s, wdx_r, hid_s, hid_r,
    rsc_s, rsc_r, ret_s, ret_r, q_s, q_r, kv_s, kv_r, o_s, o_r,
):
    ep = lax.axis_index("ep")
    tp = lax.axis_index("tp")
    z, x = lax.div(ep, NX), lax.rem(ep, NX)
    y, core = lax.div(tp, 2), lax.rem(tp, 2)
    mate = (ep, y * 2 + 1 - core)

    def ring(i, d):
        return lax.rem(i + d + RING, RING)

    y_next = ((ep, ring(y, 1) * 2 + core), (ep, ring(y, -1) * 2 + core))
    z_next = ((ring(z, 1) * NX + x, tp), (ring(z, -1) * NX + x, tp))

    def ep_peer(k):
        return lax.rem(ep + k, N_EP)

    def x_peer(k):
        return z * NX + lax.rem(x + k, NX)

    def rdma(src, dst, ssem, rsem, dev):
        return pltpu.make_async_remote_copy(
            src_ref=src, dst_ref=dst, send_sem=ssem, recv_sem=rsem,
            device_id=dev, device_id_type=MESH,
        )

    def took(ref, sem):
        rdma(ref, ref, sem, sem, mate).wait_recv()

    barrier = pltpu.get_barrier_semaphore()

    def greet(k, carry):
        pl.semaphore_signal(barrier, inc=1, device_id=(ep_peer(k + N_EP // 2), tp), device_id_type=MESH)
        return carry

    lax.fori_loop(0, N_EP // 2, greet, 0)
    lax.fori_loop(N_EP // 2 + 1, N_EP, greet, 0)
    for dev in (*y_next, mate):
        pl.semaphore_signal(barrier, inc=1, device_id=dev, device_id_type=MESH)
    for k in range(NX, 128 // 8):
        srecv[k] = jnp.zeros((8, ROWS_A), F32)

    def load(src, dst, sem):
        copy = pltpu.make_async_copy(src, dst, sem)
        copy.start()
        return copy

    tok_load = load(tok_in, tok, small_sem.at[0])
    loads_routes = load(routes_in, routes, small_sem.at[6])
    loads_mg = load(mg_in, mg, small_sem.at[4])
    loads_q = load(q_in, qall.at[x], small_sem.at[1])
    loads_k = load(k_in, kv.at[z, :, pl.ds(0, 256)], small_sem.at[2])
    loads_v = load(v_in, kv.at[z, :, pl.ds(256, 256)], small_sem.at[3])
    loads_scores = load(rs_in, scores, small_sem.at[7])
    loads_hg = load(hg_in, hg, small_sem.at[5])
    loads_lam = load(lam_in, lam, small_sem.at[8])
    load_wg = load(wg_in.at[0], wgu.at[:, pl.ds(0, FFL)], wsem.at[0])
    load_wu = load(wu_in.at[0], wgu.at[:, pl.ds(FFL, FFL)], wsem.at[1])

    def wd_cols(yd, c):
        return wd_in.at[0, :, pl.ds(pl.multiple_of((yd * 2 + c) * FEAT, FEAT), FEAT)]

    wd_loads = [load(wd_cols(yd, core), wdx.at[core, yd], wsem.at[2 + yd]) for yd in range(RING)]

    loads_routes.wait()
    r0, r1 = routes[0:1, :], routes[1:2, :]
    sub = lax.broadcasted_iota(jnp.int32, (N_EP, ROWS_B), 0)
    hit0, hit1 = sub == r0, sub == r1
    named = jnp.where(hit0 | hit1, 1.0, 0.0).astype(BF16)
    row_i = lax.broadcasted_iota(jnp.int32, (ROWS_B, ROWS_B), 0)
    col_i = lax.broadcasted_iota(jnp.int32, (ROWS_B, ROWS_B), 1)
    earlier = jnp.where(row_i < col_i, 1.0, 0.0).astype(BF16)
    before = jnp.dot(named, earlier, preferred_element_type=F32)
    pos0 = jnp.sum(jnp.where(hit0, before, 0.0), axis=0, keepdims=True)
    pos1 = jnp.sum(jnp.where(hit1, before, 0.0), axis=0, keepdims=True)
    slot0 = r0.astype(F32) * CAP + pos0
    slot1 = r1.astype(F32) * CAP + pos1
    slot_sub = lax.broadcasted_iota(jnp.int32, (SLOTS, ROWS_B), 0).astype(F32)
    pick0[...] = jnp.where(slot_sub == slot0, 1.0, 0.0).astype(BF16)
    pick1[...] = jnp.where(slot_sub == slot1, 1.0, 0.0).astype(BF16)

    tok_load.wait()
    loads_mg.wait()
    squares = jnp.zeros((ROWS_B, 256), F32)
    for i in range(D // 256):
        part = tok[:, i * 256:(i + 1) * 256].astype(F32)
        squares = squares + part * part
    mean = jnp.sum(squares, axis=1, keepdims=True) * (1.0 / D)
    inv = lax.rsqrt(mean + moe_eps)
    picks = pick0[...] + pick1[...]

    def sorted_rows(rel):
        cols = pl.ds(pl.multiple_of((ring(y, rel) * 2 + core) * FEAT, FEAT), FEAT)
        normed = (tok[:, cols].astype(F32) * inv * mg[:, cols]).astype(BF16)
        rows = jnp.dot(picks, normed, preferred_element_type=F32)
        return rows.reshape(N_EP, CAP, FEAT).astype(BF16)

    outbox[...] = sorted_rows(0)
    pl.semaphore_wait(barrier, N_EP - 1 + 3)

    def off_of(source_z, dest_z):
        return lax.rem(lax.div(source_z, 2) - lax.div(dest_z, 2) + SUB, SUB)

    def far_side(off):
        return lax.div(off, 2)

    def dispatch(k, carry):
        peer = ep_peer(k)
        off = off_of(z, lax.div(peer, NX))
        rdma(outbox.at[peer], inbox.at[ep], disp_s, disp_r.at[off], (peer, tp)).start()
        return carry

    lax.fori_loop(1, N_EP, dispatch, 0)
    inbox[ep] = outbox[ep]

    loads_q.wait()
    q_copies = [rdma(qall.at[x], qall.at[x], q_s, q_r.at[k - 1], (x_peer(k), tp)) for k in range(1, NX)]
    for copy in q_copies:
        copy.start()
    for yd in range(RING):
        rdma(wd_cols(yd, 1 - core), wdx.at[core, yd], wdx_s, wdx_r, mate).start()

    for i, rel in enumerate((4, 3, 5)):
        outfar[i] = sorted_rows(rel)

    def dispatch_far(k, carry):
        peer = ep_peer(k)
        off = off_of(z, lax.div(peer, NX))
        rdma(outfar.at[0, peer], infar.at[ep, 0], far_s, far_r.at[off], (peer, tp)).start()
        rdma(outfar.at[1 + far_side(off), peer], infar.at[ep, 1], far_s, far_r.at[off], (peer, tp)).start()
        return carry

    lax.fori_loop(1, N_EP, dispatch_far, 0)
    infar[ep, 0] = outfar[0, ep]
    infar[ep, 1] = outfar[1, ep]

    loads_k.wait()
    loads_v.wait()

    def travels(way, off):
        return (off < 2) == (way == 0)

    def kv_moves(way, d, j):
        return d < 4 or (j < KSUB // 2) == (way == 0)

    def kv_copy(way, d, j):
        origin = ring(z, -(d - 1) if way == 0 else d - 1)
        piece = kv.at[origin, pl.ds(j * KROWS, KROWS)]
        return rdma(piece, piece, kv_s, kv_r.at[way, d - 1, j], z_next[way])

    for j in range(KSUB):
        for way in range(2):
            kv_copy(way, 1, j).start()

    def kv_step(d):
        for j in range(KSUB):
            for way in range(2):
                if kv_moves(way, d, j):
                    kv_copy(way, d, j).wait_recv()
                    if d < 4 and kv_moves(way, d + 1, j):
                        kv_copy(way, d + 1, j).start()

    ORDER = (0, 3, 1, 2)

    def rows_of(off):
        return pl.ds(off * SROWS, SROWS)

    def group(off):
        return lax.rem(lax.div(z, 2) + off, SUB) * GSRC

    def gath_piece(rel, off):
        return gath.at[ring(y, rel) * 2 + core, rows_of(off)]

    def ag_copy(way, d, off):
        piece = gath_piece(-(d - 1) if way == 0 else d - 1, off)
        return rdma(piece, piece, ag_s, ag_r.at[way, d - 1, off], y_next[way])

    def to_mate(rel, off, stage):
        piece = gath_piece(rel, off)
        rdma(piece, piece, dd_s, dd_r.at[stage], mate).start()

    def flat(rows):
        return rows.astype(F32).reshape(SROWS, FEAT).astype(BF16)

    for off in ORDER:
        took(inbox.at[pl.ds(0, GSRC - 1 if off == 0 else GSRC)], disp_r.at[off])
        gath[tp, off * SROWS:(off + 1) * SROWS, :] = flat(inbox[pl.ds(group(off), GSRC)])
        for way in range(2):
            ag_copy(way, 1, off).start()
        to_mate(0, off, 0)

    def ag_step(d, off):
        for way in range(2):
            if d < 3 or travels(way, off):
                ag_copy(way, d, off).wait_recv()
                if d == 1 or (d == 2 and travels(way, off)):
                    ag_copy(way, d + 1, off).start()
                to_mate(-d if way == 0 else d, off, d - 1 if d < 3 else 2 + off)

    for off in ORDER:
        ag_step(1, off)
    for off in ORDER:
        ag_step(2, off)
    load_wg.wait()
    load_wu.wait()

    def product(rel, rows):
        terms = []
        for c in range(2):
            t = ring(y, rel) * 2 + c
            weights = wgu[pl.ds(pl.multiple_of(t * FEAT, FEAT), FEAT), :]
            terms.append(jnp.dot(gath[t, rows, :], weights, preferred_element_type=F32))
        return terms[0] + terms[1]

    every = slice(0, SLOTS)
    took(gath.at[pl.ds(0, 3)], dd_r.at[0])
    acts[...] = product(0, every) + product(1, every) + product(-1, every)
    for off in ORDER:
        took(infar.at[pl.ds(0, GSRC - 1 if off == 0 else GSRC)], far_r.at[off])
        sources = pl.ds(group(off), GSRC)
        for i, rel in ((0, 4), (1, 3 if off < 2 else -3)):
            gath[ring(y, rel) * 2 + core, off * SROWS:(off + 1) * SROWS, :] = flat(infar[sources, i])
            to_mate(rel, off, 1)
    kv_step(1)
    took(gath.at[pl.ds(0, 4)], dd_r.at[1])
    acts[...] += product(2, every) + product(-2, every) + product(4, every)
    lower, upper = slice(0, SLOTS // 2), slice(SLOTS // 2, SLOTS)
    acts[lower, :] += product(3, lower)
    acts[upper, :] += product(-3, upper)

    def hid_copy(off):
        piece = hid.at[core, rows_of(off)]
        return rdma(piece, piece, hid_s, hid_r.at[off], mate)

    def expert(off):
        took(gath.at[0, rows_of(off)], dd_r.at[2 + off])
        rows = slice(off * SROWS, (off + 1) * SROWS)
        acc = acts[rows, :] + product(-3 if off < 2 else 3, rows)
        gate_act, up_act = acc[:, :FFL], acc[:, FFL:]
        hid[core, rows, :] = (gate_act * jax.nn.sigmoid(gate_act) * up_act).astype(BF16)
        hid_copy(off).start()

    def rel_of(way, r):
        return r % RING if way == 0 else (RING - r) % RING

    def rs_copy(way, r, off):
        return rdma(
            sbuf.at[way, r - 1, rows_of(off)], rbuf.at[way, r - 1, rows_of(off)],
            rsc_s, rsc_r.at[way, r - 1, off], y_next[way],
        )

    def rs_send(way, r, off):
        rows = slice(off * SROWS, (off + 1) * SROWS)
        term = zown[rel_of(way, r), rows, :]
        if r < 3 or (r == 3 and travels(way, off)):
            rs_copy(way, r + 1, off).wait_recv()
            term = term + rbuf[way, r, rows, :].astype(F32)
        sbuf[way, r - 1, rows, :] = term.astype(BF16)
        rs_copy(way, r, off).start()

    def own_terms(rows, rels):
        hid0, hid1 = hid[0, rows, :], hid[1, rows, :]
        for rel in rels:
            yd = ring(y, rel)
            zown[rel, rows, :] = jnp.dot(hid0, wdx[0, yd], preferred_element_type=F32) + jnp.dot(
                hid1, wdx[1, yd], preferred_element_type=F32
            )

    def launch(off):
        hid_copy(off).wait_recv()
        long_way = 0 if off < 2 else 1
        own_terms(slice(off * SROWS, (off + 1) * SROWS), (4, 3, 5))
        rs_send(long_way, 4, off)
        rs_send(1 - long_way, 3, off)

    ag_step(3, ORDER[0])
    ag_step(3, ORDER[1])
    expert(ORDER[0])
    ag_step(3, ORDER[2])
    expert(ORDER[1])
    for copy in wd_loads:
        copy.wait()
    took(wdx.at[0], wdx_r)
    ag_step(3, ORDER[3])
    launch(ORDER[0])
    expert(ORDER[2])
    launch(ORDER[1])
    expert(ORDER[3])
    launch(ORDER[2])
    kv_step(2)
    launch(ORDER[3])
    own_terms(every, (2, 6))

    def attend(xq, m):
        qm = qall[xq, :, m * QKD:(m + 1) * QKD]
        keys = kv[:, :, m * QKD:(m + 1) * QKD].reshape(RING * ROWS_A, QKD)
        vals = kv[:, :, 256:512].reshape(RING * ROWS_A, VD)
        s = lax.dot_general(qm, keys, (((1,), (1,)), ((), ())), preferred_element_type=F32) * QKD ** (-0.5)
        col = lax.broadcasted_iota(jnp.int32, s.shape, 1)
        row = lax.broadcasted_iota(jnp.int32, s.shape, 0)
        key_pos = (col >> 7) * (NX * ROWS_A) + x * ROWS_A + (col & 127)
        visible = key_pos <= row + (z * NX + xq) * ROWS_A
        s = jnp.where(visible, s, neg_big)
        top = jnp.max(s, axis=1, keepdims=True)
        w = jnp.where(visible, jnp.exp(s - top), 0.0)
        total = jnp.sum(w, axis=1, keepdims=True)
        o = jnp.dot(w.astype(BF16), vals, preferred_element_type=F32)
        return o, top, total

    def attend_block(k):
        xq = lax.rem(x + k, NX)
        o0, m0, l0 = attend(xq, 0)
        osend[k, :, 0:VD] = o0.astype(BF16)
        o1, m1, l1 = attend(xq, 1)
        osend[k, :, VD:2 * VD] = o1.astype(BF16)
        sl = lax.broadcasted_iota(jnp.int32, (ROWS_A, 128), 1)
        stats = jnp.where(sl == 0, m0, jnp.where(sl == 1, l0, jnp.where(sl == 2, m1, l1)))
        ssend[k] = stats.T[0:8, :]

    def o_copies(k):
        dev = (x_peer(k), tp)
        return (
            rdma(osend.at[k], orecv.at[k - 1], o_s.at[0], o_r.at[0, k - 1], dev),
            rdma(ssend.at[k], srecv.at[k], o_s.at[1], o_r.at[1, k - 1], dev),
        )

    def attend_step(k):
        attend_block(k)
        if k > 0:
            for copy in o_copies(k):
                copy.start()

    for off in ORDER:
        rs_send(0 if off < 2 else 1, 3, off)
    own_terms(every, (1, 7, 0))
    kv_step(3)
    LATER = (3, 1, 2, 0)
    for off in LATER:
        for way in range(2):
            rs_send(way, 2, off)
    kv_step(4)
    for copy in q_copies:
        copy.wait_recv()
    attend_step(2)
    for off in LATER[:2]:
        for way in range(2):
            rs_send(way, 1, off)
    attend_step(1)
    for off in LATER[2:]:
        for way in range(2):
            rs_send(way, 1, off)
    attend_step(3)

    for off in LATER:
        rows = slice(off * SROWS, (off + 1) * SROWS)
        rs_copy(0, 1, off).wait_recv()
        rs_copy(1, 1, off).wait_recv()
        result = zown[0, rows, :] + rbuf[0, 0, rows, :].astype(F32) + rbuf[1, 0, rows, :].astype(F32)
        ebox[off * GSRC:(off + 1) * GSRC] = result.reshape(GSRC, CAP, FEAT).astype(BF16)
        first = group(off)
        for i in range(GSRC):
            peer = first + i
            if off > 0:
                rdma(ebox.at[off * GSRC + i], retbox.at[ep], ret_s, ret_r, (peer, tp)).start()
            else:

                @pl.when(peer != ep)
                def _():
                    rdma(ebox.at[off * GSRC + i], retbox.at[ep], ret_s, ret_r, (peer, tp)).start()

    retbox[ep] = ebox[lax.rem(ep, GSRC)]
    attend_step(0)

    for k in range(1, NX):
        for copy in o_copies(k):
            copy.wait_recv()

    srecv[0] = ssend[0]
    stats = srecv[...].reshape(128, ROWS_A).T

    def joined(m):
        tops = [stats[:, 8 * k + 2 * m:8 * k + 2 * m + 1] for k in range(NX)]
        sums = [stats[:, 8 * k + 2 * m + 1:8 * k + 2 * m + 2] for k in range(NX)]
        outs = [osend[0, :, m * VD:(m + 1) * VD]] + [orecv[k, :, m * VD:(m + 1) * VD] for k in range(NX - 1)]
        top = jnp.maximum(jnp.maximum(tops[0], tops[1]), jnp.maximum(tops[2], tops[3]))
        scale = [jnp.exp(t - top) for t in tops]
        total = sum(f * s for f, s in zip(scale, sums))
        return sum(f * o.astype(F32) for f, o in zip(scale, outs)) / total

    loads_hg.wait()
    loads_lam.wait()
    mixed = joined(0) - lam[0] * joined(1)
    power = jnp.mean(mixed * mixed, axis=1, keepdims=True)
    att_out[...] = (mixed * lax.rsqrt(power + head_eps) * hg[...] * head_scale).astype(BF16)
    loads_scores.wait()
    s0, s1 = scores[0:1, :], scores[1:2, :]
    smax = jnp.maximum(s0, s1)
    e0, e1 = jnp.exp(s0 - smax), jnp.exp(s1 - smax)
    esum = e0 + e1
    same = row_i == col_i
    g0 = jnp.sum(jnp.where(same, e0 / esum, 0.0), axis=1, keepdims=True)
    g1 = jnp.sum(jnp.where(same, e1 / esum, 0.0), axis=1, keepdims=True)

    took(inbox.at[pl.ds(0, N_EP - 1)], disp_s)
    took(infar.at[pl.ds(0, N_EP - 1)], far_s)
    took(qall.at[pl.ds(0, NX - 1)], q_s)
    took(wdx.at[0], wdx_s)
    took(hid.at[0], hid_s)
    took(gath.at[pl.ds(0, 5)], ag_s)
    took(gath.at[pl.ds(0, RING)], dd_s)
    took(gath.at[pl.ds(0, 7)], rsc_s)
    took(gath.at[pl.ds(0, 7)], kv_s)
    took(osend.at[pl.ds(0, NX - 1)], o_s.at[0])
    took(ssend.at[pl.ds(0, NX - 1)], o_s.at[1])
    took(ebox.at[pl.ds(0, N_EP - 1)], ret_s)

    took(retbox.at[pl.ds(0, N_EP - 1)], ret_r)
    back = retbox[...].astype(F32).reshape(SLOTS, FEAT).astype(BF16)
    contract = (((0,), (0,)), ((), ()))
    first = lax.dot_general(pick0[...], back, contract, preferred_element_type=F32)
    second = lax.dot_general(pick1[...], back, contract, preferred_element_type=F32)
    exp_out[...] = (g0 * first + g1 * second).astype(BF16)


def local(
    queries, key_rows, values, lambdas, head_gain, tokens, moe_gain, routes, route_scores, w_gate, w_up, w_down,
):
    hbm = pl.BlockSpec(memory_space=pltpu.HBM)
    vmem = pl.BlockSpec(memory_space=pltpu.VMEM)
    dma = pltpu.SemaphoreType.DMA
    boxes = (N_EP, CAP, FEAT)
    scratch = [
        pltpu.VMEM((ROWS_B, D), BF16),
        pltpu.SMEM((1,), F32),
        pltpu.VMEM((1, D), F32),
        pltpu.VMEM((1, VD), F32),
        pltpu.VMEM((2, ROWS_B), jnp.int32),
        pltpu.VMEM((2, ROWS_B), F32),
        pltpu.VMEM((SLOTS, ROWS_B), BF16),
        pltpu.VMEM((SLOTS, ROWS_B), BF16),
        dma((9,)),
        dma((2 + RING,)),
        pltpu.VMEM(boxes, BF16),
        pltpu.VMEM((3, *boxes), BF16),
        pltpu.VMEM(boxes, BF16),
        pltpu.VMEM((N_EP, 2, CAP, FEAT), BF16),
        pltpu.VMEM((N_TP, SLOTS, FEAT), BF16),
        pltpu.VMEM((SLOTS, 2 * FFL), F32),
        pltpu.VMEM((D, 2 * FFL), BF16),
        pltpu.VMEM((2, RING, FFL, FEAT), BF16),
        pltpu.VMEM((2, SLOTS, FFL), BF16),
        pltpu.VMEM((RING, SLOTS, FEAT), F32),
        pltpu.VMEM((2, 4, SLOTS, FEAT), BF16),
        pltpu.VMEM((2, 4, SLOTS, FEAT), BF16),
        pltpu.VMEM(boxes, BF16),
        pltpu.VMEM(boxes, BF16),
        pltpu.VMEM((NX, ROWS_A, 2 * QKD), BF16),
        pltpu.VMEM((RING, ROWS_A, 512), BF16),
        pltpu.VMEM((NX, ROWS_A, 2 * VD), BF16),
        pltpu.VMEM((NX, 8, ROWS_A), F32),
        pltpu.VMEM((NX - 1, ROWS_A, 2 * VD), BF16),
        pltpu.VMEM((128 // 8, 8, ROWS_A), F32),
        dma, dma((SUB,)),
        dma, dma((SUB,)),
        dma, dma((2, 3, SUB)),
        dma, dma((2 + SUB,)),
        dma, dma,
        dma, dma((SUB,)),
        dma, dma((2, 4, SUB)),
        dma, dma,
        dma, dma((NX - 1,)),
        dma, dma((2, 4, KSUB)),
        dma((2,)), dma((2, NX - 1)),
    ]
    return pl.pallas_call(
        kernel,
        out_shape=(
            pltpu.VMEM((ROWS_A, VD), BF16),
            pltpu.VMEM((ROWS_B, FEAT), BF16),
        ),
        in_specs=[hbm, hbm, hbm, hbm, hbm, hbm, hbm, hbm, hbm, hbm, hbm, hbm],
        out_specs=(vmem, vmem),
        scratch_shapes=scratch,
        compiler_params=pltpu.CompilerParams(
            collective_id=0, has_side_effects=True, vmem_limit_bytes=63000000
        ),
    )(
        queries, key_rows, values, lambdas, head_gain.reshape(1, VD), tokens,
        moe_gain.reshape(1, D), routes.T, route_scores.T, w_gate, w_up, w_down,
    )


def solution(mesh):
    return jax.shard_map(
        local,
        mesh=mesh,
        in_specs=(
            P("ep", "tp"), P("ep", "tp"), P("ep", "tp"), P("tp"), P(), P("ep", None), P(),
            P("ep", None), P("ep", None), P("ep", None, "tp"), P("ep", None, "tp"), P("ep", "tp", None),
        ),
        out_specs=(P("ep", "tp"), P("ep", "tp")),
        check_vma=False,
    )
```

```python
import jax
import jax.numpy as jnp
from jax import lax
from jax.experimental import pallas as pl
from jax.experimental.pallas import tpu as pltpu
from jax.sharding import PartitionSpec as P

MESH = pl.DeviceIdType.MESH
F32 = jnp.float32
BF16 = jnp.bfloat16

QKD = 128
VD = 256
D = 4096
N_EP = 32
N_TP = 16
NX = 4
RING = 8
CAP = 8
ROWS_A = 128
ROWS_B = 64
SLOTS = N_EP * CAP
FEAT = D // N_TP
FFL = 128
SUB = 4
SROWS = SLOTS // SUB
GSRC = N_EP // SUB
KSUB = 2
KROWS = ROWS_A // KSUB

neg_big = -1e30
head_eps = 1e-05
moe_eps = 1e-06
head_scale = 0.8


def kernel(
    q_in, k_in, v_in, lam_in, hg_in, tok_in, mg_in, routes_in, rs_in, wg_in, wu_in, wd_in,
    att_out, exp_out,
    tok, lam, mg, hg, routes, scores, pick0, pick1, small_sem, wsem,
    outbox, outfar, inbox, infar, gath, acts, wgu, wdx, hid, zown, sbuf, rbuf,
    ebox, retbox, qall, kv, osend, ssend, orecv, srecv,
    disp_s, disp_r, far_s, far_r, ag_s, ag_r, dd_s, dd_r, wdx_s, wdx_r, hid_s, hid_r,
    rsc_s, rsc_r, ret_s, ret_r, q_s, q_r, kv_s, kv_r, o_s, o_r,
):
    ep = lax.axis_index("ep")
    tp = lax.axis_index("tp")
    z, x = lax.div(ep, NX), lax.rem(ep, NX)
    y, core = lax.div(tp, 2), lax.rem(tp, 2)
    mate = (ep, y * 2 + 1 - core)

    def ring(i, d):
        return lax.rem(i + d + RING, RING)

    y_next = ((ep, ring(y, 1) * 2 + core), (ep, ring(y, -1) * 2 + core))
    z_next = ((ring(z, 1) * NX + x, tp), (ring(z, -1) * NX + x, tp))

    def ep_peer(k):
        return lax.rem(ep + k, N_EP)

    def x_peer(k):
        return z * NX + lax.rem(x + k, NX)

    def rdma(src, dst, ssem, rsem, dev):
        return pltpu.make_async_remote_copy(
            src_ref=src, dst_ref=dst, send_sem=ssem, recv_sem=rsem,
            device_id=dev, device_id_type=MESH,
        )

    def took(ref, sem):
        rdma(ref, ref, sem, sem, mate).wait_recv()

    barrier = pltpu.get_barrier_semaphore()

    def greet(k, carry):
        pl.semaphore_signal(barrier, inc=1, device_id=(ep_peer(k + N_EP // 2), tp), device_id_type=MESH)
        return carry

    lax.fori_loop(0, N_EP // 2, greet, 0)
    lax.fori_loop(N_EP // 2 + 1, N_EP, greet, 0)
    for dev in (*y_next, mate):
        pl.semaphore_signal(barrier, inc=1, device_id=dev, device_id_type=MESH)
    for k in range(NX, 128 // 8):
        srecv[k] = jnp.zeros((8, ROWS_A), F32)

    def load(src, dst, sem):
        copy = pltpu.make_async_copy(src, dst, sem)
        copy.start()
        return copy

    tok_load = load(tok_in, tok, small_sem.at[0])
    loads_routes = load(routes_in, routes, small_sem.at[6])
    loads_mg = load(mg_in, mg, small_sem.at[4])
    loads_q = load(q_in, qall.at[x], small_sem.at[1])
    loads_k = load(k_in, kv.at[z, :, pl.ds(0, 256)], small_sem.at[2])
    loads_v = load(v_in, kv.at[z, :, pl.ds(256, 256)], small_sem.at[3])
    loads_scores = load(rs_in, scores, small_sem.at[7])
    loads_hg = load(hg_in, hg, small_sem.at[5])
    loads_lam = load(lam_in, lam, small_sem.at[8])
    load_wg = load(wg_in.at[0], wgu.at[:, pl.ds(0, FFL)], wsem.at[0])
    load_wu = load(wu_in.at[0], wgu.at[:, pl.ds(FFL, FFL)], wsem.at[1])

    def wd_cols(yd, c):
        return wd_in.at[0, :, pl.ds(pl.multiple_of((yd * 2 + c) * FEAT, FEAT), FEAT)]

    wd_loads = [load(wd_cols(yd, core), wdx.at[core, yd], wsem.at[2 + yd]) for yd in range(RING)]

    loads_routes.wait()
    r0, r1 = routes[0:1, :], routes[1:2, :]
    sub = lax.broadcasted_iota(jnp.int32, (N_EP, ROWS_B), 0)
    hit0, hit1 = sub == r0, sub == r1
    named = jnp.where(hit0 | hit1, 1.0, 0.0).astype(BF16)
    row_i = lax.broadcasted_iota(jnp.int32, (ROWS_B, ROWS_B), 0)
    col_i = lax.broadcasted_iota(jnp.int32, (ROWS_B, ROWS_B), 1)
    earlier = jnp.where(row_i < col_i, 1.0, 0.0).astype(BF16)
    before = jnp.dot(named, earlier, preferred_element_type=F32)
    pos0 = jnp.sum(jnp.where(hit0, before, 0.0), axis=0, keepdims=True)
    pos1 = jnp.sum(jnp.where(hit1, before, 0.0), axis=0, keepdims=True)
    slot0 = r0.astype(F32) * CAP + pos0
    slot1 = r1.astype(F32) * CAP + pos1
    slot_sub = lax.broadcasted_iota(jnp.int32, (SLOTS, ROWS_B), 0).astype(F32)
    pick0[...] = jnp.where(slot_sub == slot0, 1.0, 0.0).astype(BF16)
    pick1[...] = jnp.where(slot_sub == slot1, 1.0, 0.0).astype(BF16)

    tok_load.wait()
    loads_mg.wait()
    squares = jnp.zeros((ROWS_B, 256), F32)
    for i in range(D // 256):
        part = tok[:, i * 256:(i + 1) * 256].astype(F32)
        squares = squares + part * part
    mean = jnp.sum(squares, axis=1, keepdims=True) * (1.0 / D)
    inv = lax.rsqrt(mean + moe_eps)
    picks = pick0[...] + pick1[...]

    def sorted_rows(rel):
        cols = pl.ds(pl.multiple_of((ring(y, rel) * 2 + core) * FEAT, FEAT), FEAT)
        normed = (tok[:, cols].astype(F32) * inv * mg[:, cols]).astype(BF16)
        rows = jnp.dot(picks, normed, preferred_element_type=F32)
        return rows.reshape(N_EP, CAP, FEAT).astype(BF16)

    outbox[...] = sorted_rows(0)
    pl.semaphore_wait(barrier, N_EP - 1 + 3)

    my_group = lax.div(z, 2)
    my_side = lax.rem(my_group, 2)
    my_off = my_side * 2 + lax.div(my_group, 2)

    def dispatch(k, carry):
        peer = ep_peer(k)
        rdma(outbox.at[peer], inbox.at[ep], disp_s, disp_r.at[my_off], (peer, tp)).start()
        return carry

    lax.fori_loop(1, N_EP, dispatch, 0)
    inbox[ep] = outbox[ep]

    loads_k.wait()
    loads_v.wait()

    def travels(way, off):
        return (off < 2) == (way == 0)

    def kv_moves(way, d, j):
        return d < 4 or (j < KSUB // 2) == (way == 0)

    def kv_copy(way, d, j):
        origin = ring(z, -(d - 1) if way == 0 else d - 1)
        piece = kv.at[origin, pl.ds(j * KROWS, KROWS)]
        return rdma(piece, piece, kv_s, kv_r.at[way, d - 1, j], z_next[way])

    for j in range(KSUB):
        for way in range(2):
            kv_copy(way, 1, j).start()

    for i, rel in enumerate((4, 3, 5)):
        outfar[i] = sorted_rows(rel)

    def dispatch_far(k, carry):
        peer = ep_peer(k)
        rdma(outfar.at[0, peer], infar.at[ep, 0], far_s, far_r.at[my_off], (peer, tp)).start()
        rdma(outfar.at[1 + my_side, peer], infar.at[ep, 1], far_s, far_r.at[my_off], (peer, tp)).start()
        return carry

    lax.fori_loop(1, N_EP, dispatch_far, 0)
    infar[ep, 0] = outfar[0, ep]
    infar[ep, 1] = outfar[1 + my_side, ep]

    def kv_step(d):
        for j in range(KSUB):
            for way in range(2):
                if kv_moves(way, d, j):
                    kv_copy(way, d, j).wait_recv()
                    if d < 4 and kv_moves(way, d + 1, j):
                        kv_copy(way, d + 1, j).start()

    ORDER = (0, 2, 1, 3)
    GROUPS = (0, 2, 1, 3)

    def rows_of(off):
        return pl.ds(off * SROWS, SROWS)

    def group(off):
        return GROUPS[off] * GSRC

    def arrived(box, sem, off):
        @pl.when(my_off == off)
        def _():
            took(box.at[pl.ds(0, GSRC - 1)], sem.at[off])

        @pl.when(my_off != off)
        def _():
            took(box.at[pl.ds(0, GSRC)], sem.at[off])

    def gath_piece(rel, off):
        return gath.at[ring(y, rel) * 2 + core, rows_of(off)]

    def ag_copy(way, d, off):
        piece = gath_piece(-(d - 1) if way == 0 else d - 1, off)
        return rdma(piece, piece, ag_s, ag_r.at[way, d - 1, off], y_next[way])

    def to_mate(rel, off, stage):
        piece = gath_piece(rel, off)
        rdma(piece, piece, dd_s, dd_r.at[stage], mate).start()

    def flat(rows):
        return rows.astype(F32).reshape(SROWS, FEAT).astype(BF16)

    for off in ORDER:
        arrived(inbox, disp_r, off)
        gath[tp, off * SROWS:(off + 1) * SROWS, :] = flat(inbox[pl.ds(group(off), GSRC)])
        for way in range(2):
            ag_copy(way, 1, off).start()
        to_mate(0, off, 0)

    def ag_step(d, off):
        for way in range(2):
            if d < 3 or travels(way, off):
                ag_copy(way, d, off).wait_recv()
                if d == 1 or (d == 2 and travels(way, off)):
                    ag_copy(way, d + 1, off).start()
                to_mate(-d if way == 0 else d, off, d - 1 if d < 3 else 2 + off)

    for off in ORDER:
        ag_step(1, off)
    kv_step(1)
    loads_q.wait()
    q_copies = [rdma(qall.at[x], qall.at[x], q_s, q_r.at[k - 1], (x_peer(k), tp)) for k in range(1, NX)]
    for copy in q_copies:
        copy.start()
    for yd in range(RING):
        rdma(wd_cols(yd, 1 - core), wdx.at[core, yd], wdx_s, wdx_r, mate).start()
    for off in ORDER:
        ag_step(2, off)
    load_wg.wait()
    load_wu.wait()

    def product(rel, rows):
        terms = []
        for c in range(2):
            t = ring(y, rel) * 2 + c
            weights = wgu[pl.ds(pl.multiple_of(t * FEAT, FEAT), FEAT), :]
            terms.append(jnp.dot(gath[t, rows, :], weights, preferred_element_type=F32))
        return terms[0] + terms[1]

    every = slice(0, SLOTS)
    took(gath.at[pl.ds(0, 3)], dd_r.at[0])
    acts[...] = product(0, every) + product(1, every) + product(-1, every)
    for off in ORDER:
        arrived(infar, far_r, off)
        sources = pl.ds(group(off), GSRC)
        for i, rel in ((0, 4), (1, 3 if off < 2 else -3)):
            gath[ring(y, rel) * 2 + core, off * SROWS:(off + 1) * SROWS, :] = flat(infar[sources, i])
            to_mate(rel, off, 1)
    took(gath.at[pl.ds(0, 4)], dd_r.at[1])
    acts[...] += product(2, every) + product(-2, every) + product(4, every)
    lower, upper = slice(0, SLOTS // 2), slice(SLOTS // 2, SLOTS)
    acts[lower, :] += product(3, lower)
    acts[upper, :] += product(-3, upper)
    kv_step(2)

    def hid_copy(off):
        piece = hid.at[core, rows_of(off)]
        return rdma(piece, piece, hid_s, hid_r.at[off], mate)

    def expert(off):
        took(gath.at[0, rows_of(off)], dd_r.at[2 + off])
        rows = slice(off * SROWS, (off + 1) * SROWS)
        acc = acts[rows, :] + product(-3 if off < 2 else 3, rows)
        gate_act, up_act = acc[:, :FFL], acc[:, FFL:]
        hid[core, rows, :] = (gate_act * jax.nn.sigmoid(gate_act) * up_act).astype(BF16)
        hid_copy(off).start()

    def rel_of(way, r):
        return r % RING if way == 0 else (RING - r) % RING

    def rs_copy(way, r, off):
        return rdma(
            sbuf.at[way, r - 1, rows_of(off)], rbuf.at[way, r - 1, rows_of(off)],
            rsc_s, rsc_r.at[way, r - 1, off], y_next[way],
        )

    def rs_send(way, r, off):
        rows = slice(off * SROWS, (off + 1) * SROWS)
        term = zown[rel_of(way, r), rows, :]
        if r < 3 or (r == 3 and travels(way, off)):
            rs_copy(way, r + 1, off).wait_recv()
            term = term + rbuf[way, r, rows, :].astype(F32)
        sbuf[way, r - 1, rows, :] = term.astype(BF16)
        rs_copy(way, r, off).start()

    def own_terms(rows, rels):
        hid0, hid1 = hid[0, rows, :], hid[1, rows, :]
        for rel in rels:
            yd = ring(y, rel)
            zown[rel, rows, :] = jnp.dot(hid0, wdx[0, yd], preferred_element_type=F32) + jnp.dot(
                hid1, wdx[1, yd], preferred_element_type=F32
            )

    def launch(off):
        hid_copy(off).wait_recv()
        long_way = 0 if off < 2 else 1
        own_terms(slice(off * SROWS, (off + 1) * SROWS), (4, 3, 5))
        rs_send(long_way, 4, off)
        rs_send(1 - long_way, 3, off)

    ag_step(3, ORDER[0])
    ag_step(3, ORDER[1])
    expert(ORDER[0])
    ag_step(3, ORDER[2])
    expert(ORDER[1])
    for copy in wd_loads:
        copy.wait()
    took(wdx.at[0], wdx_r)
    ag_step(3, ORDER[3])
    launch(ORDER[0])
    expert(ORDER[2])
    launch(ORDER[1])
    expert(ORDER[3])
    launch(ORDER[2])
    launch(ORDER[3])
    kv_step(3)
    own_terms(every, (2, 6))

    def attend(k, blocks):
        xq = lax.rem(x + k, NX)
        vals = kv[0:blocks, :, 256:512].reshape(blocks * ROWS_A, VD)
        col = lax.broadcasted_iota(jnp.int32, (ROWS_A, blocks * ROWS_A), 1)
        row = lax.broadcasted_iota(jnp.int32, (ROWS_A, blocks * ROWS_A), 0)
        key_pos = (col >> 7) * (NX * ROWS_A) + (col & 127)
        visible = key_pos - row <= (z * NX + xq - x) * ROWS_A
        stats = []
        for m in range(2):
            qm = qall[xq, :, m * QKD:(m + 1) * QKD]
            keys = kv[0:blocks, :, m * QKD:(m + 1) * QKD].reshape(blocks * ROWS_A, QKD)
            s = lax.dot_general(qm, keys, (((1,), (1,)), ((), ())), preferred_element_type=F32) * QKD ** (-0.5)
            s = jnp.where(visible, s, neg_big)
            top = jnp.max(s, axis=1, keepdims=True)
            w = jnp.exp(s - top)
            stats += [top, jnp.sum(w, axis=1, keepdims=True)]
            o = jnp.dot(w.astype(BF16), vals, preferred_element_type=F32)
            osend[k, :, m * VD:(m + 1) * VD] = o.astype(BF16)
        sl = lax.broadcasted_iota(jnp.int32, (ROWS_A, 128), 1)
        packed = jnp.where(sl == 0, stats[0], jnp.where(sl == 1, stats[1], jnp.where(sl == 2, stats[2], stats[3])))
        ssend[k] = packed.T[0:8, :]

    def attend_both(k):
        @pl.when(z < RING // 2)
        def _():
            attend(k, RING // 2)

        @pl.when(z >= RING // 2)
        def _():
            attend(k, RING)

    def o_copies(k):
        dev = (x_peer(k), tp)
        return (
            rdma(osend.at[k], orecv.at[k - 1], o_s.at[0], o_r.at[0, k - 1], dev),
            rdma(ssend.at[k], srecv.at[k], o_s.at[1], o_r.at[1, k - 1], dev),
        )

    def send_half(k):
        for copy in o_copies(k):
            copy.start()

    def attend_for(k):
        attend_both(k)
        send_half(k)

    for off in ORDER[:2]:
        rs_send(0 if off < 2 else 1, 3, off)
    own_terms(every, (1, 7, 0))
    for off in ORDER[2:]:
        rs_send(0 if off < 2 else 1, 3, off)
    for i, off in enumerate(ORDER):
        for way in range(2):
            rs_send(way, 2, off)
        if i == 2:
            kv_step(4)
            for copy in q_copies:
                copy.wait_recv()
            attend_for(2)
    for i, off in enumerate(ORDER):
        for way in range(2):
            rs_send(way, 1, off)
        if i == 0:
            attend_for(1)
        if i == 2:
            attend_for(3)

    for off in ORDER:
        rows = slice(off * SROWS, (off + 1) * SROWS)
        rs_copy(0, 1, off).wait_recv()
        rs_copy(1, 1, off).wait_recv()
        result = zown[0, rows, :] + rbuf[0, 0, rows, :].astype(F32) + rbuf[1, 0, rows, :].astype(F32)
        ebox[off * GSRC:(off + 1) * GSRC] = result.reshape(GSRC, CAP, FEAT).astype(BF16)
        first = group(off)
        for i in range(GSRC):
            peer = first + i

            @pl.when(peer != ep)
            def _():
                rdma(ebox.at[off * GSRC + i], retbox.at[ep], ret_s, ret_r, (peer, tp)).start()

    retbox[ep] = ebox[my_off * GSRC + lax.rem(ep, GSRC)]
    attend_both(0)

    for k in range(1, NX):
        for copy in o_copies(k):
            copy.wait_recv()

    srecv[0] = ssend[0]
    stats = srecv[...].reshape(128, ROWS_A).T

    def joined(m):
        tops = [stats[:, 8 * k + 2 * m:8 * k + 2 * m + 1] for k in range(NX)]
        sums = [stats[:, 8 * k + 2 * m + 1:8 * k + 2 * m + 2] for k in range(NX)]
        outs = [osend[0, :, m * VD:(m + 1) * VD]] + [orecv[k, :, m * VD:(m + 1) * VD] for k in range(NX - 1)]
        top = jnp.maximum(jnp.maximum(tops[0], tops[1]), jnp.maximum(tops[2], tops[3]))
        scale = [jnp.exp(t - top) for t in tops]
        total = sum(f * s for f, s in zip(scale, sums))
        return sum(f * o.astype(F32) for f, o in zip(scale, outs)) / total

    loads_hg.wait()
    loads_lam.wait()
    mixed = joined(0) - lam[0] * joined(1)
    power = jnp.mean(mixed * mixed, axis=1, keepdims=True)
    att_out[...] = (mixed * lax.rsqrt(power + head_eps) * hg[...] * head_scale).astype(BF16)
    loads_scores.wait()
    s0, s1 = scores[0:1, :], scores[1:2, :]
    smax = jnp.maximum(s0, s1)
    e0, e1 = jnp.exp(s0 - smax), jnp.exp(s1 - smax)
    esum = e0 + e1
    same = row_i == col_i
    g0 = jnp.sum(jnp.where(same, e0 / esum, 0.0), axis=1, keepdims=True)
    g1 = jnp.sum(jnp.where(same, e1 / esum, 0.0), axis=1, keepdims=True)

    took(inbox.at[pl.ds(0, N_EP - 1)], disp_s)
    took(infar.at[pl.ds(0, N_EP - 1)], far_s)
    took(qall.at[pl.ds(0, NX - 1)], q_s)
    took(wdx.at[0], wdx_s)
    took(hid.at[0], hid_s)
    took(gath.at[pl.ds(0, 5)], ag_s)
    took(gath.at[pl.ds(0, RING)], dd_s)
    took(gath.at[pl.ds(0, 7)], rsc_s)
    took(gath.at[pl.ds(0, 7)], kv_s)
    took(osend.at[pl.ds(0, NX - 1)], o_s.at[0])
    took(ssend.at[pl.ds(0, NX - 1)], o_s.at[1])
    took(ebox.at[pl.ds(0, N_EP - 1)], ret_s)

    took(retbox.at[pl.ds(0, N_EP - 1)], ret_r)
    back = retbox[...].astype(F32).reshape(SLOTS, FEAT).astype(BF16)
    contract = (((0,), (0,)), ((), ()))
    first = lax.dot_general(pick0[...], back, contract, preferred_element_type=F32)
    second = lax.dot_general(pick1[...], back, contract, preferred_element_type=F32)
    exp_out[...] = (g0 * first + g1 * second).astype(BF16)


def local(
    queries, key_rows, values, lambdas, head_gain, tokens, moe_gain, routes, route_scores, w_gate, w_up, w_down,
):
    hbm = pl.BlockSpec(memory_space=pltpu.HBM)
    vmem = pl.BlockSpec(memory_space=pltpu.VMEM)
    dma = pltpu.SemaphoreType.DMA
    boxes = (N_EP, CAP, FEAT)
    scratch = [
        pltpu.VMEM((ROWS_B, D), BF16),
        pltpu.SMEM((1,), F32),
        pltpu.VMEM((1, D), F32),
        pltpu.VMEM((1, VD), F32),
        pltpu.VMEM((2, ROWS_B), jnp.int32),
        pltpu.VMEM((2, ROWS_B), F32),
        pltpu.VMEM((SLOTS, ROWS_B), BF16),
        pltpu.VMEM((SLOTS, ROWS_B), BF16),
        dma((9,)),
        dma((2 + RING,)),
        pltpu.VMEM(boxes, BF16),
        pltpu.VMEM((3, *boxes), BF16),
        pltpu.VMEM(boxes, BF16),
        pltpu.VMEM((N_EP, 2, CAP, FEAT), BF16),
        pltpu.VMEM((N_TP, SLOTS, FEAT), BF16),
        pltpu.VMEM((SLOTS, 2 * FFL), F32),
        pltpu.VMEM((D, 2 * FFL), BF16),
        pltpu.VMEM((2, RING, FFL, FEAT), BF16),
        pltpu.VMEM((2, SLOTS, FFL), BF16),
        pltpu.VMEM((RING, SLOTS, FEAT), F32),
        pltpu.VMEM((2, 4, SLOTS, FEAT), BF16),
        pltpu.VMEM((2, 4, SLOTS, FEAT), BF16),
        pltpu.VMEM(boxes, BF16),
        pltpu.VMEM(boxes, BF16),
        pltpu.VMEM((NX, ROWS_A, 2 * QKD), BF16),
        pltpu.VMEM((RING, ROWS_A, 512), BF16),
        pltpu.VMEM((NX, ROWS_A, 2 * VD), BF16),
        pltpu.VMEM((NX, 8, ROWS_A), F32),
        pltpu.VMEM((NX - 1, ROWS_A, 2 * VD), BF16),
        pltpu.VMEM((128 // 8, 8, ROWS_A), F32),
        dma, dma((SUB,)),
        dma, dma((SUB,)),
        dma, dma((2, 3, SUB)),
        dma, dma((2 + SUB,)),
        dma, dma,
        dma, dma((SUB,)),
        dma, dma((2, 4, SUB)),
        dma, dma,
        dma, dma((NX - 1,)),
        dma, dma((2, 4, KSUB)),
        dma((2,)), dma((2, NX - 1)),
    ]
    return pl.pallas_call(
        kernel,
        out_shape=(
            pltpu.VMEM((ROWS_A, VD), BF16),
            pltpu.VMEM((ROWS_B, FEAT), BF16),
        ),
        in_specs=[hbm, hbm, hbm, hbm, hbm, hbm, hbm, hbm, hbm, hbm, hbm, hbm],
        out_specs=(vmem, vmem),
        scratch_shapes=scratch,
        compiler_params=pltpu.CompilerParams(
            collective_id=0, has_side_effects=True, vmem_limit_bytes=63000000
        ),
    )(
        queries, key_rows, values, lambdas, head_gain.reshape(1, VD), tokens,
        moe_gain.reshape(1, D), routes.T, route_scores.T, w_gate, w_up, w_down,
    )


def solution(mesh):
    return jax.shard_map(
        local,
        mesh=mesh,
        in_specs=(
            P("ep", "tp"), P("ep", "tp"), P("ep", "tp"), P("tp"), P(), P("ep", None), P(),
            P("ep", None), P("ep", None), P("ep", None, "tp"), P("ep", None, "tp"), P("ep", "tp", None),
        ),
        out_specs=(P("ep", "tp"), P("ep", "tp")),
        check_vma=False,
    )
```

```python
import jax
import jax.numpy as jnp
from jax import lax
from jax.experimental import pallas as pl
from jax.experimental.pallas import tpu as pltpu
from jax.sharding import PartitionSpec as P

MESH = pl.DeviceIdType.MESH
F32 = jnp.float32
BF16 = jnp.bfloat16

QKD = 128
VD = 256
D = 4096
N_EP = 32
N_TP = 16
NX = 4
RING = 8
CAP = 8
ROWS_A = 128
ROWS_B = 64
SLOTS = N_EP * CAP
FEAT = D // N_TP
FFL = 128
SUB = 4
SROWS = SLOTS // SUB
GSRC = N_EP // SUB
KSUB = 2
KROWS = ROWS_A // KSUB

neg_big = -1e30
head_eps = 1e-05
moe_eps = 1e-06
head_scale = 0.8


def kernel(
    q_in, k_in, v_in, lam_in, hg_in, tok_in, mg_in, routes_in, rs_in, wg_in, wu_in, wd_in,
    att_out, exp_out,
    tok, lam, mg, hg, routes, scores, pick0, pick1, small_sem, wsem,
    outbox, outfar, inbox, infar, gath, acts, wgu, wdx, hid, zown, sbuf, rbuf,
    ebox, retbox, qall, kv, osend, ssend, orecv, srecv,
    disp_s, disp_r, far_s, far_r, ag_s, ag_r, dd_s, dd_r, wdx_s, wdx_r, hid_s, hid_r,
    rsc_s, rsc_r, ret_s, ret_r, q_s, q_r, kv_s, kv_r, o_s, o_r,
):
    ep = lax.axis_index("ep")
    tp = lax.axis_index("tp")
    z, x = lax.div(ep, NX), lax.rem(ep, NX)
    y, core = lax.div(tp, 2), lax.rem(tp, 2)
    mate = (ep, y * 2 + 1 - core)

    def ring(i, d):
        return lax.rem(i + d + RING, RING)

    y_next = ((ep, ring(y, 1) * 2 + core), (ep, ring(y, -1) * 2 + core))
    z_next = ((ring(z, 1) * NX + x, tp), (ring(z, -1) * NX + x, tp))

    def ep_peer(k):
        return lax.rem(ep + k, N_EP)

    def x_peer(k):
        return z * NX + lax.rem(x + k, NX)

    def rdma(src, dst, ssem, rsem, dev):
        return pltpu.make_async_remote_copy(
            src_ref=src, dst_ref=dst, send_sem=ssem, recv_sem=rsem,
            device_id=dev, device_id_type=MESH,
        )

    def took(ref, sem):
        rdma(ref, ref, sem, sem, mate).wait_recv()

    barrier = pltpu.get_barrier_semaphore()

    for k in [*range(N_EP // 2, N_EP), *range(1, N_EP // 2)]:
        pl.semaphore_signal(barrier, inc=1, device_id=(ep_peer(k), tp), device_id_type=MESH)
    for dev in (*y_next, mate):
        pl.semaphore_signal(barrier, inc=1, device_id=dev, device_id_type=MESH)
    for k in range(NX, 128 // 8):
        srecv[k] = jnp.zeros((8, ROWS_A), F32)

    def load(src, dst, sem):
        copy = pltpu.make_async_copy(src, dst, sem)
        copy.start()
        return copy

    tok_load = load(tok_in, tok, small_sem.at[0])
    loads_routes = load(routes_in, routes, small_sem.at[6])
    loads_mg = load(mg_in, mg, small_sem.at[4])
    loads_q = load(q_in, qall.at[x], small_sem.at[1])
    loads_k = load(k_in, kv.at[z, :, pl.ds(0, 256)], small_sem.at[2])
    loads_v = load(v_in, kv.at[z, :, pl.ds(256, 256)], small_sem.at[3])
    loads_scores = load(rs_in, scores, small_sem.at[7])
    loads_hg = load(hg_in, hg, small_sem.at[5])
    loads_lam = load(lam_in, lam, small_sem.at[8])
    load(wg_in.at[0], wgu.at[:, pl.ds(0, FFL)], wsem.at[0])
    load(wu_in.at[0], wgu.at[:, pl.ds(FFL, FFL)], wsem.at[0])

    def wd_cols(yd, c):
        return wd_in.at[0, :, pl.ds(pl.multiple_of((yd * 2 + c) * FEAT, FEAT), FEAT)]

    for yd in range(RING):
        load(wd_cols(yd, core), wdx.at[core, yd], wsem.at[1])

    loads_routes.wait()
    r0, r1 = routes[0:1, :], routes[1:2, :]
    sub = lax.broadcasted_iota(jnp.int32, (N_EP, ROWS_B), 0)
    hit0, hit1 = sub == r0, sub == r1
    named = jnp.where(hit0 | hit1, 1.0, 0.0).astype(BF16)
    row_i = lax.broadcasted_iota(jnp.int32, (ROWS_B, ROWS_B), 0)
    col_i = lax.broadcasted_iota(jnp.int32, (ROWS_B, ROWS_B), 1)
    earlier = jnp.where(row_i < col_i, 1.0, 0.0).astype(BF16)
    before = jnp.dot(named, earlier, preferred_element_type=F32)
    pos0 = jnp.sum(jnp.where(hit0, before, 0.0), axis=0, keepdims=True)
    pos1 = jnp.sum(jnp.where(hit1, before, 0.0), axis=0, keepdims=True)
    slot0 = r0.astype(F32) * CAP + pos0
    slot1 = r1.astype(F32) * CAP + pos1
    slot_sub = lax.broadcasted_iota(jnp.int32, (SLOTS, ROWS_B), 0).astype(F32)
    pick0[...] = jnp.where(slot_sub == slot0, 1.0, 0.0).astype(BF16)
    pick1[...] = jnp.where(slot_sub == slot1, 1.0, 0.0).astype(BF16)

    tok_load.wait()
    loads_mg.wait()
    squares = jnp.zeros((ROWS_B, 256), F32)
    for i in range(D // 256):
        part = tok[:, i * 256:(i + 1) * 256].astype(F32)
        squares = squares + part * part
    mean = jnp.sum(squares, axis=1, keepdims=True) * (1.0 / D)
    inv = lax.rsqrt(mean + moe_eps)
    picks = pick0[...] + pick1[...]

    def sorted_rows(rel):
        cols = pl.ds(pl.multiple_of((ring(y, rel) * 2 + core) * FEAT, FEAT), FEAT)
        normed = (tok[:, cols].astype(F32) * inv * mg[:, cols]).astype(BF16)
        rows = jnp.dot(picks, normed, preferred_element_type=F32)
        return rows.reshape(N_EP, CAP, FEAT).astype(BF16)

    outbox[...] = sorted_rows(0)
    pl.semaphore_wait(barrier, N_EP - 1 + 3)

    my_group = lax.div(z, 2)
    my_side = lax.rem(my_group, 2)
    my_off = my_side * 2 + lax.div(my_group, 2)

    def dispatch(k, carry):
        peer = ep_peer(k)
        rdma(outbox.at[peer], inbox.at[ep], disp_s, disp_r.at[my_off], (peer, tp)).start()
        return carry

    lax.fori_loop(1, N_EP, dispatch, 0)
    inbox[ep] = outbox[ep]

    loads_k.wait()
    loads_v.wait()

    def travels(way, off):
        return (off < 2) == (way == 0)

    def kv_moves(way, d, j):
        return d < 4 or (j < KSUB // 2) == (way == 0)

    def kv_copy(way, d, j):
        origin = ring(z, -(d - 1) if way == 0 else d - 1)
        piece = kv.at[origin, pl.ds(j * KROWS, KROWS)]
        return rdma(piece, piece, kv_s, kv_r.at[way, d - 1, j], z_next[way])

    for j in range(KSUB):
        for way in range(2):
            kv_copy(way, 1, j).start()

    for i, rel in enumerate((4, 3, 5)):
        outfar[i] = sorted_rows(rel)

    def dispatch_far(k, carry):
        peer = ep_peer(k)
        rdma(outfar.at[0, peer], infar.at[ep, 0], far_s, far_r.at[my_off], (peer, tp)).start()
        rdma(outfar.at[1 + my_side, peer], infar.at[ep, 1], far_s, far_r.at[my_off], (peer, tp)).start()
        return carry

    lax.fori_loop(1, N_EP, dispatch_far, 0)
    infar[ep, 0] = outfar[0, ep]
    infar[ep, 1] = outfar[1 + my_side, ep]

    def kv_step(d):
        for j in range(KSUB):
            for way in range(2):
                if kv_moves(way, d, j):
                    kv_copy(way, d, j).wait_recv()
                    if d < 4 and kv_moves(way, d + 1, j):
                        kv_copy(way, d + 1, j).start()

    ORDER = (0, 2, 1, 3)
    GROUPS = (0, 2, 1, 3)

    def rows_of(off):
        return pl.ds(off * SROWS, SROWS)

    def group(off):
        return GROUPS[off] * GSRC

    def arrived(box, sem, off):
        @pl.when(my_off == off)
        def _():
            took(box.at[pl.ds(0, GSRC - 1)], sem.at[off])

        @pl.when(my_off != off)
        def _():
            took(box.at[pl.ds(0, GSRC)], sem.at[off])

    def gath_piece(rel, off):
        return gath.at[ring(y, rel) * 2 + core, rows_of(off)]

    def ag_copy(way, d, off):
        piece = gath_piece(-(d - 1) if way == 0 else d - 1, off)
        return rdma(piece, piece, ag_s, ag_r.at[way, d - 1, off], y_next[way])

    def to_mate(rel, off, stage):
        piece = gath_piece(rel, off)
        rdma(piece, piece, dd_s, dd_r.at[stage], mate).start()

    def flat(rows):
        return rows.astype(F32).reshape(SROWS, FEAT).astype(BF16)

    for off in ORDER:
        arrived(inbox, disp_r, off)
        gath[tp, off * SROWS:(off + 1) * SROWS, :] = flat(inbox[pl.ds(group(off), GSRC)])
        for way in range(2):
            ag_copy(way, 1, off).start()
        to_mate(0, off, 0)

    def ag_step(d, off):
        for way in range(2):
            if d < 3 or travels(way, off):
                ag_copy(way, d, off).wait_recv()
                if d == 1 or (d == 2 and travels(way, off)):
                    ag_copy(way, d + 1, off).start()
                to_mate(-d if way == 0 else d, off, d - 1 if d < 3 else 2 + off)

    for off in ORDER:
        ag_step(1, off)
    kv_step(1)
    loads_q.wait()
    q_copies = [rdma(qall.at[x], qall.at[x], q_s, q_r.at[k - 1], (x_peer(k), tp)) for k in range(1, NX)]
    for copy in q_copies:
        copy.start()
    for yd in range(RING):
        rdma(wd_cols(yd, 1 - core), wdx.at[core, yd], wdx_s, wdx_r, mate).start()
    for off in ORDER:
        ag_step(2, off)
    took(gath, wsem.at[0])

    def product(rel, rows):
        terms = []
        for c in range(2):
            t = ring(y, rel) * 2 + c
            weights = wgu[pl.ds(pl.multiple_of(t * FEAT, FEAT), FEAT), :]
            terms.append(jnp.dot(gath[t, rows, :], weights, preferred_element_type=F32))
        return terms[0] + terms[1]

    every = slice(0, SLOTS)
    took(gath.at[pl.ds(0, 3)], dd_r.at[0])
    acts[...] = product(0, every) + product(1, every) + product(-1, every)
    for off in ORDER:
        arrived(infar, far_r, off)
        sources = pl.ds(group(off), GSRC)
        for i, rel in ((0, 4), (1, 3 if off < 2 else -3)):
            gath[ring(y, rel) * 2 + core, off * SROWS:(off + 1) * SROWS, :] = flat(infar[sources, i])
            to_mate(rel, off, 1)
    took(gath.at[pl.ds(0, 4)], dd_r.at[1])
    acts[...] += product(2, every) + product(-2, every) + product(4, every)
    lower, upper = slice(0, SLOTS // 2), slice(SLOTS // 2, SLOTS)
    acts[lower, :] += product(3, lower)
    acts[upper, :] += product(-3, upper)
    kv_step(2)

    def hid_copy(off):
        piece = hid.at[core, rows_of(off)]
        return rdma(piece, piece, hid_s, hid_r.at[off], mate)

    def expert(off):
        took(gath.at[0, rows_of(off)], dd_r.at[2 + off])
        rows = slice(off * SROWS, (off + 1) * SROWS)
        acc = acts[rows, :] + product(-3 if off < 2 else 3, rows)
        gate_act, up_act = acc[:, :FFL], acc[:, FFL:]
        hid[core, rows, :] = (gate_act * jax.nn.sigmoid(gate_act) * up_act).astype(BF16)
        hid_copy(off).start()

    def rel_of(way, r):
        return r % RING if way == 0 else (RING - r) % RING

    def rs_copy(way, r, off):
        return rdma(
            sbuf.at[way, r - 1, rows_of(off)], rbuf.at[way, r - 1, rows_of(off)],
            rsc_s, rsc_r.at[way, r - 1, off], y_next[way],
        )

    def rs_send(way, r, off):
        rows = slice(off * SROWS, (off + 1) * SROWS)
        term = zown[rel_of(way, r), rows, :]
        if r < 3 or (r == 3 and travels(way, off)):
            rs_copy(way, r + 1, off).wait_recv()
            term = term + rbuf[way, r, rows, :].astype(F32)
        sbuf[way, r - 1, rows, :] = term.astype(BF16)
        rs_copy(way, r, off).start()

    def own_terms(rows, rels):
        hid0, hid1 = hid[0, rows, :], hid[1, rows, :]
        for rel in rels:
            yd = ring(y, rel)
            zown[rel, rows, :] = jnp.dot(hid0, wdx[0, yd], preferred_element_type=F32) + jnp.dot(
                hid1, wdx[1, yd], preferred_element_type=F32
            )

    def launch(off):
        hid_copy(off).wait_recv()
        long_way = 0 if off < 2 else 1
        own_terms(slice(off * SROWS, (off + 1) * SROWS), (4, 3, 5))
        rs_send(long_way, 4, off)
        rs_send(1 - long_way, 3, off)

    ag_step(3, ORDER[0])
    ag_step(3, ORDER[1])
    expert(ORDER[0])
    ag_step(3, ORDER[2])
    expert(ORDER[1])
    took(wdx.at[0], wsem.at[1])
    took(wdx.at[0], wdx_r)
    ag_step(3, ORDER[3])
    launch(ORDER[0])
    expert(ORDER[2])
    launch(ORDER[1])
    expert(ORDER[3])
    launch(ORDER[2])
    launch(ORDER[3])
    kv_step(3)
    own_terms(every, (2, 6))

    def attend(k, blocks):
        xq = lax.rem(x + k, NX)
        vals = kv[0:blocks, :, 256:512].reshape(blocks * ROWS_A, VD)
        col = lax.broadcasted_iota(jnp.int32, (ROWS_A, blocks * ROWS_A), 1)
        row = lax.broadcasted_iota(jnp.int32, (ROWS_A, blocks * ROWS_A), 0)
        key_pos = (col >> 7) * (NX * ROWS_A) + (col & 127)
        visible = key_pos - row <= (z * NX + xq - x) * ROWS_A
        stats = []
        for m in range(2):
            qm = qall[xq, :, m * QKD:(m + 1) * QKD]
            keys = kv[0:blocks, :, m * QKD:(m + 1) * QKD].reshape(blocks * ROWS_A, QKD)
            s = lax.dot_general(qm, keys, (((1,), (1,)), ((), ())), preferred_element_type=F32) * QKD ** (-0.5)
            s = jnp.where(visible, s, neg_big)
            top = jnp.max(s, axis=1, keepdims=True)
            w = jnp.exp(s - top)
            stats += [top, jnp.sum(w, axis=1, keepdims=True)]
            o = jnp.dot(w.astype(BF16), vals, preferred_element_type=F32)
            osend[k, :, m * VD:(m + 1) * VD] = o.astype(BF16)
        sl = lax.broadcasted_iota(jnp.int32, (ROWS_A, 128), 1)
        packed = jnp.where(sl == 0, stats[0], jnp.where(sl == 1, stats[1], jnp.where(sl == 2, stats[2], stats[3])))
        ssend[k] = packed.T[0:8, :]

    def attend_both(k):
        @pl.when(z < RING // 2)
        def _():
            attend(k, RING // 2)

        @pl.when(z >= RING // 2)
        def _():
            attend(k, RING)

    def o_copies(k):
        dev = (x_peer(k), tp)
        return (
            rdma(osend.at[k], orecv.at[k - 1], o_s.at[0], o_r.at[0, k - 1], dev),
            rdma(ssend.at[k], srecv.at[k], o_s.at[1], o_r.at[1, k - 1], dev),
        )

    def send_half(k):
        for copy in o_copies(k):
            copy.start()

    def attend_for(k):
        attend_both(k)
        send_half(k)

    for off in ORDER[:2]:
        rs_send(0 if off < 2 else 1, 3, off)
    own_terms(every, (1, 7, 0))
    for off in ORDER[2:]:
        rs_send(0 if off < 2 else 1, 3, off)
    for i, off in enumerate(ORDER):
        for way in range(2):
            rs_send(way, 2, off)
        if i == 2:
            kv_step(4)
            for copy in q_copies:
                copy.wait_recv()
            attend_for(2)
    for i, off in enumerate(ORDER):
        for way in range(2):
            rs_send(way, 1, off)
        if i == 0:
            attend_for(1)
        if i == 2:
            attend_for(3)

    for off in ORDER:
        rows = slice(off * SROWS, (off + 1) * SROWS)
        rs_copy(0, 1, off).wait_recv()
        rs_copy(1, 1, off).wait_recv()
        result = zown[0, rows, :] + rbuf[0, 0, rows, :].astype(F32) + rbuf[1, 0, rows, :].astype(F32)
        ebox[off * GSRC:(off + 1) * GSRC] = result.reshape(GSRC, CAP, FEAT).astype(BF16)
        first = group(off)
        for i in range(GSRC):
            peer = first + i

            @pl.when(peer != ep)
            def _():
                rdma(ebox.at[off * GSRC + i], retbox.at[ep], ret_s, ret_r, (peer, tp)).start()

    retbox[ep] = ebox[my_off * GSRC + lax.rem(ep, GSRC)]
    attend_both(0)

    for k in range(1, NX):
        for copy in o_copies(k):
            copy.wait_recv()

    srecv[0] = ssend[0]
    stats = srecv[...].reshape(128, ROWS_A).T

    def joined(m):
        tops = [stats[:, 8 * k + 2 * m:8 * k + 2 * m + 1] for k in range(NX)]
        sums = [stats[:, 8 * k + 2 * m + 1:8 * k + 2 * m + 2] for k in range(NX)]
        outs = [osend[0, :, m * VD:(m + 1) * VD]] + [orecv[k, :, m * VD:(m + 1) * VD] for k in range(NX - 1)]
        top = jnp.maximum(jnp.maximum(tops[0], tops[1]), jnp.maximum(tops[2], tops[3]))
        scale = [jnp.exp(t - top) for t in tops]
        total = sum(f * s for f, s in zip(scale, sums))
        return sum(f * o.astype(F32) for f, o in zip(scale, outs)) / total

    loads_hg.wait()
    loads_lam.wait()
    mixed = joined(0) - lam[0] * joined(1)
    power = jnp.mean(mixed * mixed, axis=1, keepdims=True)
    att_out[...] = (mixed * lax.rsqrt(power + head_eps) * hg[...] * head_scale).astype(BF16)
    loads_scores.wait()
    s0, s1 = scores[0:1, :], scores[1:2, :]
    smax = jnp.maximum(s0, s1)
    e0, e1 = jnp.exp(s0 - smax), jnp.exp(s1 - smax)
    esum = e0 + e1
    same = row_i == col_i
    g0 = jnp.sum(jnp.where(same, e0 / esum, 0.0), axis=1, keepdims=True)
    g1 = jnp.sum(jnp.where(same, e1 / esum, 0.0), axis=1, keepdims=True)

    took(inbox.at[pl.ds(0, N_EP - 1)], disp_s)
    took(infar.at[pl.ds(0, N_EP - 1)], far_s)
    took(qall.at[pl.ds(0, NX - 1)], q_s)
    took(wdx.at[0], wdx_s)
    took(hid.at[0], hid_s)
    took(gath.at[pl.ds(0, 5)], ag_s)
    took(gath.at[pl.ds(0, RING)], dd_s)
    took(gath.at[pl.ds(0, 7)], rsc_s)
    took(gath.at[pl.ds(0, 7)], kv_s)
    took(osend.at[pl.ds(0, NX - 1)], o_s.at[0])
    took(ssend.at[pl.ds(0, NX - 1)], o_s.at[1])
    took(ebox.at[pl.ds(0, N_EP - 1)], ret_s)

    took(retbox.at[pl.ds(0, N_EP - 1)], ret_r)
    back = retbox[...].astype(F32).reshape(SLOTS, FEAT).astype(BF16)
    contract = (((0,), (0,)), ((), ()))
    first = lax.dot_general(pick0[...], back, contract, preferred_element_type=F32)
    second = lax.dot_general(pick1[...], back, contract, preferred_element_type=F32)
    exp_out[...] = (g0 * first + g1 * second).astype(BF16)


def local(
    queries, key_rows, values, lambdas, head_gain, tokens, moe_gain, routes, route_scores, w_gate, w_up, w_down,
):
    hbm = pl.BlockSpec(memory_space=pltpu.HBM)
    vmem = pl.BlockSpec(memory_space=pltpu.VMEM)
    dma = pltpu.SemaphoreType.DMA
    boxes = (N_EP, CAP, FEAT)
    scratch = [
        pltpu.VMEM((ROWS_B, D), BF16),
        pltpu.SMEM((1,), F32),
        pltpu.VMEM((1, D), F32),
        pltpu.VMEM((1, VD), F32),
        pltpu.VMEM((2, ROWS_B), jnp.int32),
        pltpu.VMEM((2, ROWS_B), F32),
        pltpu.VMEM((SLOTS, ROWS_B), BF16),
        pltpu.VMEM((SLOTS, ROWS_B), BF16),
        dma((9,)),
        dma((2,)),
        pltpu.VMEM(boxes, BF16),
        pltpu.VMEM((3, *boxes), BF16),
        pltpu.VMEM(boxes, BF16),
        pltpu.VMEM((N_EP, 2, CAP, FEAT), BF16),
        pltpu.VMEM((N_TP, SLOTS, FEAT), BF16),
        pltpu.VMEM((SLOTS, 2 * FFL), F32),
        pltpu.VMEM((D, 2 * FFL), BF16),
        pltpu.VMEM((2, RING, FFL, FEAT), BF16),
        pltpu.VMEM((2, SLOTS, FFL), BF16),
        pltpu.VMEM((RING, SLOTS, FEAT), F32),
        pltpu.VMEM((2, 4, SLOTS, FEAT), BF16),
        pltpu.VMEM((2, 4, SLOTS, FEAT), BF16),
        pltpu.VMEM(boxes, BF16),
        pltpu.VMEM(boxes, BF16),
        pltpu.VMEM((NX, ROWS_A, 2 * QKD), BF16),
        pltpu.VMEM((RING, ROWS_A, 512), BF16),
        pltpu.VMEM((NX, ROWS_A, 2 * VD), BF16),
        pltpu.VMEM((NX, 8, ROWS_A), F32),
        pltpu.VMEM((NX - 1, ROWS_A, 2 * VD), BF16),
        pltpu.VMEM((128 // 8, 8, ROWS_A), F32),
        dma, dma((SUB,)),
        dma, dma((SUB,)),
        dma, dma((2, 3, SUB)),
        dma, dma((2 + SUB,)),
        dma, dma,
        dma, dma((SUB,)),
        dma, dma((2, 4, SUB)),
        dma, dma,
        dma, dma((NX - 1,)),
        dma, dma((2, 4, KSUB)),
        dma((2,)), dma((2, NX - 1)),
    ]
    return pl.pallas_call(
        kernel,
        out_shape=(
            pltpu.VMEM((ROWS_A, VD), BF16),
            pltpu.VMEM((ROWS_B, FEAT), BF16),
        ),
        in_specs=[hbm, hbm, hbm, hbm, hbm, hbm, hbm, hbm, hbm, hbm, hbm, hbm],
        out_specs=(vmem, vmem),
        scratch_shapes=scratch,
        compiler_params=pltpu.CompilerParams(
            collective_id=0, has_side_effects=True, vmem_limit_bytes=63000000
        ),
    )(
        queries, key_rows, values, lambdas, head_gain.reshape(1, VD), tokens,
        moe_gain.reshape(1, D), routes.T, route_scores.T, w_gate, w_up, w_down,
    )


def solution(mesh):
    return jax.shard_map(
        local,
        mesh=mesh,
        in_specs=(
            P("ep", "tp"), P("ep", "tp"), P("ep", "tp"), P("tp"), P(), P("ep", None), P(),
            P("ep", None), P("ep", None), P("ep", None, "tp"), P("ep", None, "tp"), P("ep", "tp", None),
        ),
        out_specs=(P("ep", "tp"), P("ep", "tp")),
        check_vma=False,
    )
```

```python
import jax
import jax.numpy as jnp
from jax import lax
from jax.experimental import pallas as pl
from jax.experimental.pallas import tpu as pltpu
from jax.sharding import PartitionSpec as P

MESH = pl.DeviceIdType.MESH
F32 = jnp.float32
BF16 = jnp.bfloat16

QKD = 128
VD = 256
D = 4096
N_EP = 32
N_TP = 16
NX = 4
RING = 8
CAP = 8
ROWS_A = 128
ROWS_B = 64
SLOTS = N_EP * CAP
FEAT = D // N_TP
FFL = 128
SUB = 4
SROWS = SLOTS // SUB
GSRC = N_EP // SUB
HROWS = SLOTS // SUB // 2
KSUB = 2
KROWS = ROWS_A // KSUB

neg_big = -1e30
head_eps = 1e-05
moe_eps = 1e-06
head_scale = 0.8


def kernel(
    q_in, k_in, v_in, lam_in, hg_in, tok_in, mg_in, routes_in, rs_in, wg_in, wu_in, wd_in,
    att_out, exp_out,
    tok, lam, mg, hg, routes, scores, pick0, pick1, small_sem, wsem,
    outbox, outfar, inbox, infar, gath, acts, wgu, wdx, hid, zown, sbuf, rbuf,
    ebox, retbox, qall, kv, osend, ssend, orecv, srecv,
    disp_s, disp_r, far_s, far_r, ag_s, ag_r, dd_s, dd_r, wdx_s, wdx_r, hid_s, hid_r,
    rsc_s, rsc_r, ret_s, ret_r, q_s, q_r, kv_s, kv_r, o_s, o_r,
):
    ep = lax.axis_index("ep")
    tp = lax.axis_index("tp")
    z, x = lax.div(ep, NX), lax.rem(ep, NX)
    y, core = lax.div(tp, 2), lax.rem(tp, 2)
    mate = (ep, y * 2 + 1 - core)

    def ring(i, d):
        return lax.rem(i + d + RING, RING)

    y_next = ((ep, ring(y, 1) * 2 + core), (ep, ring(y, -1) * 2 + core))
    z_next = ((ring(z, 1) * NX + x, tp), (ring(z, -1) * NX + x, tp))

    def ep_peer(k):
        return lax.rem(ep + k, N_EP)

    def x_peer(k):
        return z * NX + lax.rem(x + k, NX)

    def rdma(src, dst, ssem, rsem, dev):
        return pltpu.make_async_remote_copy(
            src_ref=src, dst_ref=dst, send_sem=ssem, recv_sem=rsem,
            device_id=dev, device_id_type=MESH,
        )

    def took(ref, sem):
        rdma(ref, ref, sem, sem, mate).wait_recv()

    barrier = pltpu.get_barrier_semaphore()

    for k in [*range(N_EP // 2, N_EP), *range(1, N_EP // 2)]:
        pl.semaphore_signal(barrier, inc=1, device_id=(ep_peer(k), tp), device_id_type=MESH)
    for dev in (*y_next, mate):
        pl.semaphore_signal(barrier, inc=1, device_id=dev, device_id_type=MESH)
    for k in range(NX, 128 // 8):
        srecv[k] = jnp.zeros((8, ROWS_A), F32)

    def load(src, dst, sem):
        copy = pltpu.make_async_copy(src, dst, sem)
        copy.start()
        return copy

    tok_load = load(tok_in, tok, small_sem.at[0])
    loads_routes = load(routes_in, routes, small_sem.at[6])
    loads_mg = load(mg_in, mg, small_sem.at[4])
    loads_q = load(q_in, qall.at[x], small_sem.at[1])
    loads_k = load(k_in, kv.at[z, :, pl.ds(0, 256)], small_sem.at[2])
    loads_v = load(v_in, kv.at[z, :, pl.ds(256, 256)], small_sem.at[3])
    loads_scores = load(rs_in, scores, small_sem.at[7])
    loads_hg = load(hg_in, hg, small_sem.at[5])
    loads_lam = load(lam_in, lam, small_sem.at[8])
    load(wg_in.at[0], wgu.at[:, pl.ds(0, FFL)], wsem.at[0])
    load(wu_in.at[0], wgu.at[:, pl.ds(FFL, FFL)], wsem.at[0])

    def wd_cols(yd, c):
        return wd_in.at[0, :, pl.ds(pl.multiple_of((yd * 2 + c) * FEAT, FEAT), FEAT)]

    for yd in range(RING):
        load(wd_cols(yd, core), wdx.at[core, yd], wsem.at[1])

    loads_routes.wait()
    r0, r1 = routes[0:1, :], routes[1:2, :]
    sub = lax.broadcasted_iota(jnp.int32, (N_EP, ROWS_B), 0)
    hit0, hit1 = sub == r0, sub == r1
    named = jnp.where(hit0 | hit1, 1.0, 0.0).astype(BF16)
    row_i = lax.broadcasted_iota(jnp.int32, (ROWS_B, ROWS_B), 0)
    col_i = lax.broadcasted_iota(jnp.int32, (ROWS_B, ROWS_B), 1)
    earlier = jnp.where(row_i < col_i, 1.0, 0.0).astype(BF16)
    before = jnp.dot(named, earlier, preferred_element_type=F32)
    pos0 = jnp.sum(jnp.where(hit0, before, 0.0), axis=0, keepdims=True)
    pos1 = jnp.sum(jnp.where(hit1, before, 0.0), axis=0, keepdims=True)
    slot0 = r0.astype(F32) * CAP + pos0
    slot1 = r1.astype(F32) * CAP + pos1
    slot_sub = lax.broadcasted_iota(jnp.int32, (SLOTS, ROWS_B), 0).astype(F32)
    pick0[...] = jnp.where(slot_sub == slot0, 1.0, 0.0).astype(BF16)
    pick1[...] = jnp.where(slot_sub == slot1, 1.0, 0.0).astype(BF16)

    tok_load.wait()
    loads_mg.wait()
    squares = jnp.zeros((ROWS_B, 256), F32)
    for i in range(D // 256):
        part = tok[:, i * 256:(i + 1) * 256].astype(F32)
        squares = squares + part * part
    mean = jnp.sum(squares, axis=1, keepdims=True) * (1.0 / D)
    inv = lax.rsqrt(mean + moe_eps)
    picks = pick0[...] + pick1[...]

    def sorted_rows(rel):
        cols = pl.ds(pl.multiple_of((ring(y, rel) * 2 + core) * FEAT, FEAT), FEAT)
        normed = (tok[:, cols].astype(F32) * inv * mg[:, cols]).astype(BF16)
        rows = jnp.dot(picks, normed, preferred_element_type=F32)
        return rows.reshape(N_EP, CAP, FEAT).astype(BF16)

    outbox[...] = sorted_rows(0)
    pl.semaphore_wait(barrier, N_EP - 1 + 3)

    my_group = lax.div(z, 2)
    my_side = lax.rem(my_group, 2)
    my_off = my_side * 2 + lax.div(my_group, 2)

    def dispatch(k, carry):
        peer = ep_peer(k)
        rdma(outbox.at[peer], inbox.at[ep], disp_s, disp_r.at[my_off], (peer, tp)).start()
        return carry

    lax.fori_loop(1, N_EP, dispatch, 0)
    inbox[ep] = outbox[ep]

    loads_k.wait()
    loads_v.wait()

    def travels(way, off):
        return (off < 2) == (way == 0)

    def kv_moves(way, d, j):
        return d < 4 or (j < KSUB // 2) == (way == 0)

    def kv_copy(way, d, j):
        origin = ring(z, -(d - 1) if way == 0 else d - 1)
        piece = kv.at[origin, pl.ds(j * KROWS, KROWS)]
        return rdma(piece, piece, kv_s, kv_r.at[way, d - 1, j], z_next[way])

    for j in range(KSUB):
        for way in range(2):
            kv_copy(way, 1, j).start()

    for i, rel in enumerate((4, 3, 5)):
        outfar[i] = sorted_rows(rel)

    def dispatch_far(k, carry):
        peer = ep_peer(k)
        rdma(outfar.at[0, peer], infar.at[ep, 0], far_s, far_r.at[my_off], (peer, tp)).start()
        rdma(outfar.at[1 + my_side, peer], infar.at[ep, 1], far_s, far_r.at[my_off], (peer, tp)).start()
        return carry

    lax.fori_loop(1, N_EP, dispatch_far, 0)
    infar[ep, 0] = outfar[0, ep]
    infar[ep, 1] = outfar[1 + my_side, ep]

    def kv_step(d):
        for j in range(KSUB):
            for way in range(2):
                if kv_moves(way, d, j):
                    kv_copy(way, d, j).wait_recv()
                    if d < 4 and kv_moves(way, d + 1, j):
                        kv_copy(way, d + 1, j).start()

    ORDER = (0, 2, 1, 3)
    GROUPS = (0, 2, 1, 3)

    def rows_of(off):
        return pl.ds(off * SROWS, SROWS)

    def group(off):
        return GROUPS[off] * GSRC

    def arrived(box, sem, off):
        @pl.when(my_off == off)
        def _():
            took(box.at[pl.ds(0, GSRC - 1)], sem.at[off])

        @pl.when(my_off != off)
        def _():
            took(box.at[pl.ds(0, GSRC)], sem.at[off])

    def gath_piece(rel, off):
        return gath.at[ring(y, rel) * 2 + core, rows_of(off)]

    def ag_copy(way, d, off):
        piece = gath_piece(-(d - 1) if way == 0 else d - 1, off)
        return rdma(piece, piece, ag_s, ag_r.at[way, d - 1, off], y_next[way])

    def to_mate(rel, off, stage):
        piece = gath_piece(rel, off)
        rdma(piece, piece, dd_s, dd_r.at[stage], mate).start()

    def flat(rows):
        return rows.astype(F32).reshape(SROWS, FEAT).astype(BF16)

    for off in ORDER:
        arrived(inbox, disp_r, off)
        gath[tp, off * SROWS:(off + 1) * SROWS, :] = flat(inbox[pl.ds(group(off), GSRC)])
        for way in range(2):
            ag_copy(way, 1, off).start()
        to_mate(0, off, 0)

    def ag_step(d, off):
        for way in range(2):
            if d < 3 or travels(way, off):
                ag_copy(way, d, off).wait_recv()
                if d == 1 or (d == 2 and travels(way, off)):
                    ag_copy(way, d + 1, off).start()
                to_mate(-d if way == 0 else d, off, d - 1 if d < 3 else 2 + off)

    for off in ORDER:
        ag_step(1, off)
    kv_step(1)
    loads_q.wait()
    q_copies = [rdma(qall.at[x], qall.at[x], q_s, q_r.at[k - 1], (x_peer(k), tp)) for k in range(1, NX)]
    for copy in q_copies:
        copy.start()
    for yd in range(RING):
        rdma(wd_cols(yd, 1 - core), wdx.at[core, yd], wdx_s, wdx_r, mate).start()
    for off in ORDER:
        ag_step(2, off)
    took(gath, wsem.at[0])

    def product(rel, rows):
        terms = []
        for c in range(2):
            t = ring(y, rel) * 2 + c
            weights = wgu[pl.ds(pl.multiple_of(t * FEAT, FEAT), FEAT), :]
            terms.append(jnp.dot(gath[t, rows, :], weights, preferred_element_type=F32))
        return terms[0] + terms[1]

    every = slice(0, SLOTS)
    took(gath.at[pl.ds(0, 3)], dd_r.at[0])
    acts[...] = product(0, every) + product(1, every) + product(-1, every)
    for off in ORDER:
        arrived(infar, far_r, off)
        sources = pl.ds(group(off), GSRC)
        for i, rel in ((0, 4), (1, 3 if off < 2 else -3)):
            gath[ring(y, rel) * 2 + core, off * SROWS:(off + 1) * SROWS, :] = flat(infar[sources, i])
            to_mate(rel, off, 1)
    took(gath.at[pl.ds(0, 4)], dd_r.at[1])
    acts[...] += product(2, every) + product(-2, every) + product(4, every)
    lower, upper = slice(0, SLOTS // 2), slice(SLOTS // 2, SLOTS)
    acts[lower, :] += product(3, lower)
    acts[upper, :] += product(-3, upper)
    kv_step(2)

    def hid_copy(off):
        piece = hid.at[core, rows_of(off)]
        return rdma(piece, piece, hid_s, hid_r.at[off], mate)

    def expert(off):
        took(gath.at[0, rows_of(off)], dd_r.at[2 + off])
        rows = slice(off * SROWS, (off + 1) * SROWS)
        acc = acts[rows, :] + product(-3 if off < 2 else 3, rows)
        gate_act, up_act = acc[:, :FFL], acc[:, FFL:]
        hid[core, rows, :] = (gate_act * jax.nn.sigmoid(gate_act) * up_act).astype(BF16)
        hid_copy(off).start()

    def rel_of(way, r):
        return r % RING if way == 0 else (RING - r) % RING

    def rs_copy(way, r, p):
        rows = pl.ds(p * HROWS, HROWS)
        return rdma(
            sbuf.at[way, r - 1, rows], rbuf.at[way, r - 1, rows],
            rsc_s, rsc_r.at[way, r - 1, p], y_next[way],
        )

    def rs_send(way, r, off):
        for p in (2 * off, 2 * off + 1):
            rows = slice(p * HROWS, (p + 1) * HROWS)
            term = zown[rel_of(way, r), rows, :]
            if r < 3 or (r == 3 and travels(way, off)):
                rs_copy(way, r + 1, p).wait_recv()
                term = term + rbuf[way, r, rows, :].astype(F32)
            sbuf[way, r - 1, rows, :] = term.astype(BF16)
            rs_copy(way, r, p).start()

    def own_terms(rows, rels):
        hid0, hid1 = hid[0, rows, :], hid[1, rows, :]
        for rel in rels:
            yd = ring(y, rel)
            zown[rel, rows, :] = jnp.dot(hid0, wdx[0, yd], preferred_element_type=F32) + jnp.dot(
                hid1, wdx[1, yd], preferred_element_type=F32
            )

    def launch(off):
        hid_copy(off).wait_recv()
        long_way = 0 if off < 2 else 1
        own_terms(slice(off * SROWS, (off + 1) * SROWS), (4, 3, 5))
        rs_send(long_way, 4, off)
        rs_send(1 - long_way, 3, off)

    ag_step(3, ORDER[0])
    ag_step(3, ORDER[1])
    expert(ORDER[0])
    ag_step(3, ORDER[2])
    expert(ORDER[1])
    took(wdx.at[0], wsem.at[1])
    took(wdx.at[0], wdx_r)
    ag_step(3, ORDER[3])
    launch(ORDER[0])
    expert(ORDER[2])
    launch(ORDER[1])
    expert(ORDER[3])
    launch(ORDER[2])
    launch(ORDER[3])
    kv_step(3)
    own_terms(every, (2, 6))

    def attend(k, blocks):
        xq = lax.rem(x + k, NX)
        vals = kv[0:blocks, :, 256:512].reshape(blocks * ROWS_A, VD)
        col = lax.broadcasted_iota(jnp.int32, (ROWS_A, blocks * ROWS_A), 1)
        row = lax.broadcasted_iota(jnp.int32, (ROWS_A, blocks * ROWS_A), 0)
        key_pos = (col >> 7) * (NX * ROWS_A) + (col & 127)
        visible = key_pos - row <= (z * NX + xq - x) * ROWS_A
        stats = []
        for m in range(2):
            qm = qall[xq, :, m * QKD:(m + 1) * QKD]
            keys = kv[0:blocks, :, m * QKD:(m + 1) * QKD].reshape(blocks * ROWS_A, QKD)
            s = lax.dot_general(qm, keys, (((1,), (1,)), ((), ())), preferred_element_type=F32) * QKD ** (-0.5)
            s = jnp.where(visible, s, neg_big)
            top = jnp.max(s, axis=1, keepdims=True)
            w = jnp.exp(s - top)
            stats += [top, jnp.sum(w, axis=1, keepdims=True)]
            o = jnp.dot(w.astype(BF16), vals, preferred_element_type=F32)
            osend[k, :, m * VD:(m + 1) * VD] = o.astype(BF16)
        sl = lax.broadcasted_iota(jnp.int32, (ROWS_A, 128), 1)
        packed = jnp.where(sl == 0, stats[0], jnp.where(sl == 1, stats[1], jnp.where(sl == 2, stats[2], stats[3])))
        ssend[k] = packed.T[0:8, :]

    def attend_both(k):
        @pl.when(z < RING // 2)
        def _():
            attend(k, RING // 2)

        @pl.when(z >= RING // 2)
        def _():
            attend(k, RING)

    def o_copies(k):
        dev = (x_peer(k), tp)
        return (
            rdma(osend.at[k], orecv.at[k - 1], o_s.at[0], o_r.at[0, k - 1], dev),
            rdma(ssend.at[k], srecv.at[k], o_s.at[1], o_r.at[1, k - 1], dev),
        )

    def send_half(k):
        for copy in o_copies(k):
            copy.start()

    def attend_for(k):
        attend_both(k)
        send_half(k)

    for off in ORDER[:2]:
        rs_send(0 if off < 2 else 1, 3, off)
    own_terms(every, (1, 7, 0))
    for off in ORDER[2:]:
        rs_send(0 if off < 2 else 1, 3, off)
    for i, off in enumerate(ORDER):
        for way in range(2):
            rs_send(way, 2, off)
        if i == 2:
            kv_step(4)
            for copy in q_copies:
                copy.wait_recv()
            attend_for(2)
    for i, off in enumerate(ORDER):
        for way in range(2):
            rs_send(way, 1, off)
        if i == 0:
            attend_for(1)
        if i == 2:
            attend_for(3)

    for off in ORDER:
        rows = slice(off * SROWS, (off + 1) * SROWS)
        for p in (2 * off, 2 * off + 1):
            rs_copy(0, 1, p).wait_recv()
            rs_copy(1, 1, p).wait_recv()
        result = zown[0, rows, :] + rbuf[0, 0, rows, :].astype(F32) + rbuf[1, 0, rows, :].astype(F32)
        ebox[off * GSRC:(off + 1) * GSRC] = result.reshape(GSRC, CAP, FEAT).astype(BF16)
        first = group(off)
        for i in range(GSRC):
            peer = first + i

            @pl.when(peer != ep)
            def _():
                rdma(ebox.at[off * GSRC + i], retbox.at[ep], ret_s, ret_r, (peer, tp)).start()

    retbox[ep] = ebox[my_off * GSRC + lax.rem(ep, GSRC)]
    attend_both(0)

    for k in range(1, NX):
        for copy in o_copies(k):
            copy.wait_recv()

    srecv[0] = ssend[0]
    stats = srecv[...].reshape(128, ROWS_A).T

    def joined(m):
        tops = [stats[:, 8 * k + 2 * m:8 * k + 2 * m + 1] for k in range(NX)]
        sums = [stats[:, 8 * k + 2 * m + 1:8 * k + 2 * m + 2] for k in range(NX)]
        outs = [osend[0, :, m * VD:(m + 1) * VD]] + [orecv[k, :, m * VD:(m + 1) * VD] for k in range(NX - 1)]
        top = jnp.maximum(jnp.maximum(tops[0], tops[1]), jnp.maximum(tops[2], tops[3]))
        scale = [jnp.exp(t - top) for t in tops]
        total = sum(f * s for f, s in zip(scale, sums))
        return sum(f * o.astype(F32) for f, o in zip(scale, outs)) / total

    loads_hg.wait()
    loads_lam.wait()
    mixed = joined(0) - lam[0] * joined(1)
    power = jnp.mean(mixed * mixed, axis=1, keepdims=True)
    att_out[...] = (mixed * lax.rsqrt(power + head_eps) * hg[...] * head_scale).astype(BF16)
    loads_scores.wait()
    s0, s1 = scores[0:1, :], scores[1:2, :]
    smax = jnp.maximum(s0, s1)
    e0, e1 = jnp.exp(s0 - smax), jnp.exp(s1 - smax)
    esum = e0 + e1
    same = row_i == col_i
    g0 = jnp.sum(jnp.where(same, e0 / esum, 0.0), axis=1, keepdims=True)
    g1 = jnp.sum(jnp.where(same, e1 / esum, 0.0), axis=1, keepdims=True)

    took(inbox.at[pl.ds(0, N_EP - 1)], disp_s)
    took(infar.at[pl.ds(0, N_EP - 1)], far_s)
    took(qall.at[pl.ds(0, NX - 1)], q_s)
    took(wdx.at[0], wdx_s)
    took(hid.at[0], hid_s)
    took(gath.at[pl.ds(0, 5)], ag_s)
    took(gath.at[pl.ds(0, RING)], dd_s)
    took(gath.at[pl.ds(0, 7)], rsc_s)
    took(gath.at[pl.ds(0, 7)], kv_s)
    took(osend.at[pl.ds(0, NX - 1)], o_s.at[0])
    took(ssend.at[pl.ds(0, NX - 1)], o_s.at[1])
    took(ebox.at[pl.ds(0, N_EP - 1)], ret_s)

    took(retbox.at[pl.ds(0, N_EP - 1)], ret_r)
    back = retbox[...].astype(F32).reshape(SLOTS, FEAT).astype(BF16)
    contract = (((0,), (0,)), ((), ()))
    first = lax.dot_general(pick0[...], back, contract, preferred_element_type=F32)
    second = lax.dot_general(pick1[...], back, contract, preferred_element_type=F32)
    exp_out[...] = (g0 * first + g1 * second).astype(BF16)


def local(
    queries, key_rows, values, lambdas, head_gain, tokens, moe_gain, routes, route_scores, w_gate, w_up, w_down,
):
    hbm = pl.BlockSpec(memory_space=pltpu.HBM)
    vmem = pl.BlockSpec(memory_space=pltpu.VMEM)
    dma = pltpu.SemaphoreType.DMA
    boxes = (N_EP, CAP, FEAT)
    scratch = [
        pltpu.VMEM((ROWS_B, D), BF16),
        pltpu.SMEM((1,), F32),
        pltpu.VMEM((1, D), F32),
        pltpu.VMEM((1, VD), F32),
        pltpu.VMEM((2, ROWS_B), jnp.int32),
        pltpu.VMEM((2, ROWS_B), F32),
        pltpu.VMEM((SLOTS, ROWS_B), BF16),
        pltpu.VMEM((SLOTS, ROWS_B), BF16),
        dma((9,)),
        dma((2,)),
        pltpu.VMEM(boxes, BF16),
        pltpu.VMEM((3, *boxes), BF16),
        pltpu.VMEM(boxes, BF16),
        pltpu.VMEM((N_EP, 2, CAP, FEAT), BF16),
        pltpu.VMEM((N_TP, SLOTS, FEAT), BF16),
        pltpu.VMEM((SLOTS, 2 * FFL), F32),
        pltpu.VMEM((D, 2 * FFL), BF16),
        pltpu.VMEM((2, RING, FFL, FEAT), BF16),
        pltpu.VMEM((2, SLOTS, FFL), BF16),
        pltpu.VMEM((RING, SLOTS, FEAT), F32),
        pltpu.VMEM((2, 4, SLOTS, FEAT), BF16),
        pltpu.VMEM((2, 4, SLOTS, FEAT), BF16),
        pltpu.VMEM(boxes, BF16),
        pltpu.VMEM(boxes, BF16),
        pltpu.VMEM((NX, ROWS_A, 2 * QKD), BF16),
        pltpu.VMEM((RING, ROWS_A, 512), BF16),
        pltpu.VMEM((NX, ROWS_A, 2 * VD), BF16),
        pltpu.VMEM((NX, 8, ROWS_A), F32),
        pltpu.VMEM((NX - 1, ROWS_A, 2 * VD), BF16),
        pltpu.VMEM((128 // 8, 8, ROWS_A), F32),
        dma, dma((SUB,)),
        dma, dma((SUB,)),
        dma, dma((2, 3, SUB)),
        dma, dma((2 + SUB,)),
        dma, dma,
        dma, dma((SUB,)),
        dma, dma((2, 4, 2 * SUB)),
        dma, dma,
        dma, dma((NX - 1,)),
        dma, dma((2, 4, KSUB)),
        dma((2,)), dma((2, NX - 1)),
    ]
    return pl.pallas_call(
        kernel,
        out_shape=(
            pltpu.VMEM((ROWS_A, VD), BF16),
            pltpu.VMEM((ROWS_B, FEAT), BF16),
        ),
        in_specs=[hbm, hbm, hbm, hbm, hbm, hbm, hbm, hbm, hbm, hbm, hbm, hbm],
        out_specs=(vmem, vmem),
        scratch_shapes=scratch,
        compiler_params=pltpu.CompilerParams(
            collective_id=0, has_side_effects=True, vmem_limit_bytes=63000000
        ),
    )(
        queries, key_rows, values, lambdas, head_gain.reshape(1, VD), tokens,
        moe_gain.reshape(1, D), routes.T, route_scores.T, w_gate, w_up, w_down,
    )


def solution(mesh):
    return jax.shard_map(
        local,
        mesh=mesh,
        in_specs=(
            P("ep", "tp"), P("ep", "tp"), P("ep", "tp"), P("tp"), P(), P("ep", None), P(),
            P("ep", None), P("ep", None), P("ep", None, "tp"), P("ep", None, "tp"), P("ep", "tp", None),
        ),
        out_specs=(P("ep", "tp"), P("ep", "tp")),
        check_vma=False,
    )
```
